256 devices in a mesh: ep: 64 (over z, y, core), tp: 4 (over x).
Axes of the slice: x: 4, y: 4, z: 8, core: 2. Of those that a mesh axis runs over, the one named last changes fastest.
Arguments:
- mixer_in: bfloat16 [32768, 2048], P('ep'), may hold values from -6 to 6
- mixer_gain: float32 [2048], replicated, may hold values from 0.1 to 1.9
- query_weight: bfloat16 [2048, 1024], P(None, 'tp'), may hold values from -0.125 to 0.125
- key_weight: bfloat16 [2048, 1024], P(None, 'tp'), may hold values from -0.125 to 0.125
- value_weight: bfloat16 [2048, 1024], P(None, 'tp'), may hold values from -0.125 to 0.125
- input_gate: float32 [8, 32768], P('tp', 'ep'), may hold values from -4 to 240
- forget_gate: float32 [8, 32768], P('tp', 'ep'), may hold values from 0 to 25
- head_gain: float32 [1024], replicated, may hold values from 0.1 to 1.9
- mixer_out_weight: bfloat16 [1024, 2048], P('tp'), may hold values from -0.1875 to 0.1875
- expert_in: bfloat16 [16384, 2048], P('ep'), may hold values from -6 to 6
- expert_gain: float32 [2048], replicated, may hold values from 0.1 to 1.9
- group_router: bfloat16 [2048, 16], replicated, may hold values from -0.125 to 0.125
- expert_router: bfloat16 [2048, 64], replicated, may hold values from -0.125 to 0.125
- routes: int32 [16384, 2], P('ep'), may hold values from 0 to 63, all different within a row; in each aligned block of 256 rows (0 to 255, 256 to 511, ...) at most 16 rows name the same one
- gate_experts: bfloat16 [64, 2048, 1024], P('ep', None, 'tp'), may hold values from -0.125 to 0.125
- up_experts: bfloat16 [64, 2048, 1024], P('ep', None, 'tp'), may hold values from -0.125 to 0.125
- down_experts: bfloat16 [64, 1024, 2048], P('ep', 'tp'), may hold values from -0.1875 to 0.1875
Outputs:
- mixer_out: bfloat16 [32768, 2048], P(('ep', 'tp'))
- expert_out: bfloat16 [16384, 2048], P('ep', 'tp')
The draws below stay inside these ranges and needn't reach their ends.
Inputs may be any that keep to these rules, and one draw needn't show every extreme that they name: `routes`: each row names 2 different experts. In each aligned block of 256 rows (the rows of one index of ep) no expert is named by more than 16 rows, a bound that some block reaches.
All inputs are finite; a program needn't handle non-finite values.
Results may differ from the reference program's by a relative error of at most 0.014.
The reference program's roundings to bfloat16 on the way count: a program that leaves them out, or rounds other values in their place, can miss the bound.
Values may be sent and summed in bfloat16 or wider, within the bound.
A program may use at most 128 MiB of HBM per device.

```python
import math
import jax
import jax.numpy as jnp
import numpy as np
from jax import lax

D = 2048
HEADS = 8
W = 1024
FF = 1024
BLOCK = 128
TOPK = 2
TA_DEV = 512
TB_DEV = 256
SEQUENCE_SPAN = 32768
TB = 16384
EXPERTS = 64
GROUPS = 16
CAP = 16
N_EP = 64
N_TP = 4


def draw_input_gate(key, part):
    value_rows = jnp.clip(jax.random.normal(jax.random.fold_in(key, 11), (HEADS, SEQUENCE_SPAN), jnp.float32), -4.0, 4.0)
    return value_rows


def draw_forget_gate(key, part):
    sequence_place = jnp.arange(SEQUENCE_SPAN)
    fast_cut = 5
    is_fast = jax.random.randint(jax.random.fold_in(key, 21), (HEADS,), 0, 10) < fast_cut
    factors = jnp.exp(jax.random.uniform(jax.random.fold_in(key, 22), (SEQUENCE_SPAN // TA_DEV,), jnp.float32, math.log(0.4), math.log(2.5)))
    noise = jnp.exp(0.7 * jnp.clip(jax.random.normal(jax.random.fold_in(key, 23), (HEADS, SEQUENCE_SPAN), jnp.float32), -4.0, 4.0))
    slow_rate = 0.3 / SEQUENCE_SPAN * factors[sequence_place // TA_DEV]
    rate = jnp.where(is_fast[:, None], 1.0 / 40.0, slow_rate[None, :]) * noise
    value_rows = -jnp.log(rate)
    spike_location = jax.random.randint(jax.random.fold_in(key, 25), (3,), 0, SEQUENCE_SPAN)
    retain_flag = jax.random.uniform(jax.random.fold_in(key, 26), (HEADS, 3), jnp.float32, 0.5, 0.8)
    spike_magnitude = jnp.log(retain_flag / (1.0 - retain_flag))
    for column_slot in range(3):
        value_rows = jnp.where(sequence_place[None, :] == spike_location[column_slot], spike_magnitude[:, column_slot:column_slot + 1], value_rows)
    return value_rows


def steps_of(rng, extent, shards, smallest, largest):
    level, own = 1.0, jax.random.fold_in(rng, 6)
    for dim, parts in shards:
        heights = jnp.exp(jax.random.uniform(jax.random.fold_in(own, dim), (parts,), jnp.float32, smallest / len(shards), largest / len(shards)))
        level = level * jnp.repeat(heights, extent[dim] // parts).reshape([-1 if axis == dim else 1 for axis in range(len(extent))])
    return level


def routed_block(key, own, number, rows, count, top, limit, skew):
    ranking = jax.random.permutation(key, count)
    crowded, common = shares(count, rows * top, limit, skew, True), shares(count, rows * top, limit, skew, False)
    places = jnp.arange(count)

    def named(lengths, offset_by):
        used = int((lengths > 0).sum())
        fixed = max(1, used // 4)
        shifted = fixed + (places - fixed + offset_by * (used - fixed)) % max(1, count - fixed)
        return jnp.zeros((count,), jnp.int32).at[ranking[jnp.where(places < fixed, places, shifted)]].set(jnp.asarray(lengths, jnp.int32))

    lengths = jnp.where(number % 4 == 0, named(crowded, number // 4), named(common, number - number // 4 - 1))
    mixed = jax.random.permutation(jax.random.fold_in(own, 3), count)
    source_of, sink = mixed[0:count // 2 * 2:2], mixed[1:count // 2 * 2:2]
    margin = jnp.minimum(lengths[source_of] - 1, limit - lengths[sink]) // 2
    margin = jnp.where((source_of == ranking[0]) | (sink == ranking[0]) | (lengths[sink] == 0), 0, jnp.maximum(margin, 0))
    shifted = jax.random.randint(jax.random.fold_in(own, 4), (count // 2,), 0, 1 << 20) % (margin + 1)
    lengths = lengths.at[source_of].add(-shifted).at[sink].add(shifted)
    labels = jnp.searchsorted(jnp.cumsum(lengths), jnp.arange(rows * top), side="right").astype(jnp.int32)
    table = labels.reshape(top, rows).T
    table = table[jax.random.permutation(jax.random.fold_in(own, 1), rows)]
    offset_by = jax.random.randint(jax.random.fold_in(own, 2), (rows, 1), 0, top)
    return jnp.take_along_axis(table, (jnp.arange(top)[None, :] + offset_by) % top, axis=1)


def shares(count, total, limit, slope, full):
    weights = [(1 << 20) // math.isqrt(standing ** slope) + 1 for standing in range(1, count + 1)]
    largest = limit if full else min(limit, max(-(-total // count), total * weights[0] // sum(weights)))
    least = 1 if total - largest >= count - 1 else 0
    holding, surplus = [largest] + [least] * (count - 1), total - largest - least * (count - 1)
    while surplus > 0:
        candidates = [i for i in range(1, count) if holding[i] < largest] or [i for i in range(1, count) if holding[i] < limit]
        whole, budget = sum([weights[i] for i in candidates]), surplus
        for i in candidates:
            addition = min(limit - holding[i], max(1, budget * weights[i] // whole), surplus)
            holding[i] = holding[i] + addition
            surplus = surplus - addition
    return np.array(holding)


def normal_values(key, dims, scale, bound, pieces=(), kind=jnp.bfloat16):
    entries = jax.random.normal(key, dims, jnp.float32) * scale
    if len(pieces) > 0:
        entries = steps_of(key, dims, pieces, -0.22, 0.18) * entries
    return jnp.clip(entries, min=-bound, max=bound).astype(kind)


def setup_inputs(seed: int = 0) -> dict:
    key_list = jax.random.split(jax.random.key(seed), 18)
    mixer_in = normal_values(key_list[0], (SEQUENCE_SPAN, D), 1.0, 6.0, ((0, 64),))
    mixer_gain = jnp.clip(1.0 + 0.18 * jax.random.normal(key_list[1], (D,), jnp.float32), 0.1, 1.9)
    query_weight = normal_values(key_list[2], (D, W), D ** -0.5, 0.125, ((1, 4),))
    key_weight = normal_values(key_list[3], (D, W), D ** -0.5, 0.125, ((1, 4),))
    value_weight = normal_values(key_list[4], (D, W), D ** -0.5, 0.125, ((1, 4),))
    input_gate = draw_input_gate(jax.random.fold_in(key_list[17], 71), 0)
    forget_gate = draw_forget_gate(jax.random.fold_in(key_list[17], 71), 0)
    head_gain = jnp.clip(1.0 + 0.18 * jax.random.normal(key_list[7], (W,), jnp.float32), 0.1, 1.9)
    mixer_out_weight = normal_values(key_list[8], (W, D), W ** -0.5, 0.1875, ((0, 4),))
    expert_in = normal_values(key_list[9], (TB, D), 1.0, 6.0, ((0, 64),))
    expert_gain = jnp.clip(1.0 + 0.18 * jax.random.normal(key_list[10], (D,), jnp.float32), 0.1, 1.9)
    group_router = normal_values(key_list[11], (D, GROUPS), D ** -0.5, 0.125)
    expert_router = normal_values(key_list[12], (D, EXPERTS), D ** -0.5, 0.125)
    routes_keys = jax.random.split(jax.random.fold_in(key_list[13], 1), TB // TB_DEV)
    routes_turns = jax.random.permutation(jax.random.fold_in(key_list[13], 3), TB // TB_DEV)
    routes = jax.vmap(lambda own, number: routed_block(jax.random.fold_in(key_list[13], 2), own, number, TB_DEV, EXPERTS, TOPK, CAP, 1))(routes_keys, routes_turns).reshape((TB, TOPK))
    gate_experts = normal_values(key_list[14], (EXPERTS, D, FF), D ** -0.5, 0.125, ((0, 64), (2, 4)))
    up_experts = normal_values(key_list[15], (EXPERTS, D, FF), D ** -0.5, 0.125, ((0, 64), (2, 4)))
    down_experts = normal_values(key_list[16], (EXPERTS, FF, D), FF ** -0.5, 0.1875, ((0, 64), (1, 4)))
    return dict(mixer_in=mixer_in, mixer_gain=mixer_gain, query_weight=query_weight, key_weight=key_weight, value_weight=value_weight, input_gate=input_gate, forget_gate=forget_gate, head_gain=head_gain, mixer_out_weight=mixer_out_weight, expert_in=expert_in, expert_gain=expert_gain, group_router=group_router, expert_router=expert_router, routes=routes, gate_experts=gate_experts, up_experts=up_experts, down_experts=down_experts)


epsilon = 1e-06
highest = lax.Precision.HIGHEST
floor_log = -1e+30

def rms_rows(matrix, gain):
    widened = matrix.astype(jnp.float32)
    scaled = widened * lax.rsqrt(lax.optimization_barrier(jnp.mean(widened * widened, axis=-1, keepdims=True)) + epsilon)
    return scaled * gain

def block_state(keys, value_rows, input_block, forget_block, scale):
    cumulative = jnp.cumsum(forget_block, axis=-1)
    total_log = cumulative[..., -1]
    log_weight = total_log[..., None] - cumulative + input_block
    peak_log = lax.optimization_barrier(jnp.max(log_weight, axis=-1))
    weights = jnp.exp(log_weight - peak_log[..., None])
    key_float = keys.astype(jnp.float32) * scale
    value_weighted = value_rows.astype(jnp.float32) * weights[..., None]
    memory = jnp.einsum('...sv,...sk->...vk', value_weighted, key_float, precision=highest)
    return (memory, peak_log, total_log)

def merge_state(earlier, later):
    peak_log = jnp.maximum(later[2] + earlier[1], later[1])
    fade_earlier = jnp.exp(later[2] + earlier[1] - peak_log)
    fade_later = jnp.exp(later[1] - peak_log)
    memory = fade_earlier[..., None, None] * earlier[0] + fade_later[..., None, None] * later[0]
    return (memory, peak_log, earlier[2] + later[2])

def block_out(queries, keys, value_rows, input_block, forget_block, state, scale):
    cumulative = jnp.cumsum(forget_block, axis=-1)
    length = cumulative.shape[-1]
    causal = jnp.tril(jnp.ones((length, length), dtype=bool))
    within = jnp.where(causal, cumulative[..., :, None] - cumulative[..., None, :] + input_block[..., None, :], -jnp.inf)
    carried = cumulative + state[1][..., None]
    highest_log = jnp.maximum(lax.optimization_barrier(jnp.max(within, axis=-1)), carried)
    weight_within = jnp.exp(within - highest_log[..., None])
    weight_carried = jnp.exp(carried - highest_log)
    raw_scores = jnp.einsum('...td,...sd->...ts', queries.astype(jnp.float32), keys.astype(jnp.float32)) * scale
    block_scores = raw_scores * weight_within
    rounded = lax.optimization_barrier(block_scores.astype(jnp.bfloat16)).astype(jnp.float32)
    numerator = jnp.einsum('...ts,...sd->...td', rounded, value_rows.astype(jnp.float32))
    query_float = queries.astype(jnp.float32)
    return numerator + weight_carried[..., None] * jnp.einsum('...vk,...tk->...tv', state[0], query_float, precision=highest)

def route_weights(group_logits, expert_logits, routes):
    members = expert_logits.shape[1] // group_logits.shape[1]
    chosen = jnp.take_along_axis(expert_logits, routes, axis=1)
    group_pick = jnp.take_along_axis(group_logits, routes // members, axis=1)
    return jax.nn.sigmoid(group_pick) * jax.nn.sigmoid(chosen - chosen[:, ::-1])

def reference(mixer_in, mixer_gain, query_weight, key_weight, value_weight, input_gate, forget_gate, head_gain, mixer_out_weight, expert_in, expert_gain, group_router, expert_router, routes, gate_experts, up_experts, down_experts):
    normed_a = rms_rows(mixer_in, mixer_gain).astype(jnp.bfloat16)
    queries = jnp.dot(normed_a, query_weight, preferred_element_type=jnp.float32).astype(jnp.bfloat16)
    keys = jnp.dot(normed_a, key_weight, preferred_element_type=jnp.float32).astype(jnp.bfloat16)
    value_rows = jnp.dot(normed_a, value_weight, preferred_element_type=jnp.float32).astype(jnp.bfloat16)
    sequence = normed_a.shape[0]
    head_count = input_gate.shape[0]
    width = queries.shape[1]
    head_size = width // head_count
    block_count = sequence // BLOCK
    scale = head_size ** (-0.5)

    def split_heads(matrix):
        return matrix.reshape(block_count, BLOCK, head_count, head_size).transpose(0, 2, 1, 3)

    def split_gates(gates):
        return gates.reshape(head_count, block_count, BLOCK).transpose(1, 0, 2)
    initial = (jnp.zeros((head_count, head_size, head_size), jnp.float32), jnp.full((head_count,), floor_log, jnp.float32), jnp.zeros((head_count,), jnp.float32))

    def block_step(state, block_data):
        query_block, key_block, value_block, input_block, forget_block = block_data
        output = block_out(query_block, key_block, value_block, input_block, forget_block, state, scale)
        updated = merge_state(state, block_state(key_block, value_block, input_block, forget_block, scale))
        return (updated, output)
    outcome = lax.scan(block_step, initial, (split_heads(queries), split_heads(keys), split_heads(value_rows), split_gates(input_gate), split_gates(jax.nn.log_sigmoid(forget_gate))))
    cells = outcome[1].transpose(0, 2, 1, 3).reshape(sequence, head_count, head_size)
    cell_rows = rms_rows(cells, head_gain.reshape(head_count, head_size)).reshape(sequence, width).astype(jnp.bfloat16)
    group_width = width // N_TP
    mixed = jnp.zeros((sequence, mixer_out_weight.shape[1]), jnp.float32)
    for group in range(N_TP):
        partial_value = jnp.dot(cell_rows[:, group * group_width:(group + 1) * group_width], mixer_out_weight[group * group_width:(group + 1) * group_width], preferred_element_type=jnp.float32).astype(jnp.bfloat16)
        mixed = mixed + lax.optimization_barrier(partial_value).astype(jnp.float32)
    mixer_out = mixed.astype(jnp.bfloat16)
    normed_b = rms_rows(expert_in, expert_gain).astype(jnp.bfloat16)
    group_logits = jnp.dot(normed_b, group_router, preferred_element_type=jnp.float32)
    expert_logits = jnp.dot(normed_b, expert_router, preferred_element_type=jnp.float32)
    combine = route_weights(group_logits, expert_logits, routes)
    token_count = normed_b.shape[0]
    expert_total = expert_logits.shape[1]
    token_device = token_count // N_EP
    capacity = 4 * token_device // expert_total
    flat_routes = routes.reshape(-1)
    pair_total = flat_routes.shape[0]
    matches = (flat_routes.reshape(N_EP, 2 * token_device)[:, :, None] == jnp.arange(expert_total, dtype=jnp.int32)[None, None, :]).astype(jnp.int32)
    sequence_place = (lax.optimization_barrier(jnp.sum(jnp.cumsum(matches, axis=1) * matches, axis=2)) - 1).reshape(-1)
    source = jnp.arange(pair_total, dtype=jnp.int32) // (2 * token_device)
    slot_index = source * capacity + sequence_place
    owner = jnp.full((expert_total, N_EP * capacity), pair_total, jnp.int32).at[flat_routes, slot_index].set(jnp.arange(pair_total, dtype=jnp.int32))
    padded = jnp.concatenate([normed_b, jnp.zeros((1, normed_b.shape[1]), jnp.bfloat16)], axis=0)
    weights_flat = jnp.concatenate([combine.reshape(-1), jnp.zeros((1,), jnp.float32)])
    hidden_group = gate_experts.shape[2] // N_TP

    def expert_step(total_out, expert_data):
        owners, gate_weight, up_weight, down_weight = expert_data
        rows_in = padded[owners // 2]
        gate_act = jnp.dot(rows_in, gate_weight, preferred_element_type=jnp.float32)
        up_act = jnp.dot(rows_in, up_weight, preferred_element_type=jnp.float32)
        hidden = (jax.nn.silu(gate_act) * up_act).astype(jnp.bfloat16)
        summed = jnp.zeros((rows_in.shape[0], down_weight.shape[1]), jnp.float32)
        for group in range(N_TP):
            partial_value = jnp.dot(hidden[:, group * hidden_group:(group + 1) * hidden_group], down_weight[group * hidden_group:(group + 1) * hidden_group], preferred_element_type=jnp.float32).astype(jnp.bfloat16)
            summed = summed + lax.optimization_barrier(partial_value).astype(jnp.float32)
        result = lax.optimization_barrier(summed.astype(jnp.bfloat16)).astype(jnp.float32)
        total_out = total_out.at[owners // 2].add(weights_flat[owners][:, None] * result)
        return (total_out, None)
    finished = lax.scan(expert_step, jnp.zeros((token_count + 1, normed_b.shape[1]), jnp.float32), (owner, gate_experts, up_experts, down_experts))
    expert_out = finished[0][:token_count].astype(jnp.bfloat16)
    return (mixer_out, expert_out)
```

```python
import jax
import jax.numpy as jnp
from jax import lax
from jax.sharding import Mesh
from jax.sharding import PartitionSpec as P

BLOCK = 128
EP = ("ep_0", "ep_1", "ep_2")
EP_TP = ("ep_0", "ep_1", "ep_2", "tp")


epsilon = 1e-06
highest = lax.Precision.HIGHEST
floor_log = -1e30


def filled_with(x, identity):
    return jax.tree.map(
        lambda a, e: jnp.broadcast_to(jnp.asarray(e, a.dtype), a.shape), x, identity
    )


def collected_together(x, axis):
    leaves = jax.tree.leaves(x)
    order = sorted(range(len(leaves)), key=lambda k: -leaves[k].size)
    width = (1, *leaves[order[0]].shape)[-1]
    lines = [
        jnp.pad(leaves[k].reshape(-1), (0, -leaves[k].size % width)).reshape(-1, width)
        for k in order
    ]
    both, at, found = (lax.all_gather(jnp.concatenate(lines), axis), 0, {})
    for k, line in zip(order, lines):
        slab = both[:, at : at + len(line)].reshape(len(both), -1)
        found[k] = slab[:, : leaves[k].size].reshape(-1, *leaves[k].shape)
        at += len(line)
    numbers = iter(range(len(leaves)))
    return jax.tree.map(lambda _: found[next(numbers)], x)


def prefix_by_axis(x, axes, combine, identity):
    before = start = filled_with(x, identity)
    so_far = x
    for axis in reversed(axes):
        length, place = (lax.axis_size(axis), lax.axis_index(axis))
        pieces = collected_together(so_far, axis)
        inside, so_far = (start, start)
        for k in range(length):
            passed = k < place
            so_far = combine(so_far, jax.tree.map(lambda part: part[k], pieces))
            inside = jax.tree.map(lambda new, old: jnp.where(passed, new, old), so_far, inside)
        before = combine(inside, before)
    return before


def split_up(x, dim, length):
    shape = x.shape
    parts = x.reshape(*shape[:dim], length, shape[dim] // length, *shape[dim + 1 :])
    return jnp.moveaxis(parts, dim, 0)


def sum_at_owner(x, axis, dim):
    length = lax.axis_size(axis)
    parts = lax.all_to_all(split_up(x, dim, length), axis, 0, 0, tiled=True)
    return jnp.sum(parts.astype(jnp.float32), axis=0)


def rms_rows(matrix, gain):
    widened = matrix.astype(jnp.float32)
    scaled = widened * lax.rsqrt(jnp.mean(widened * widened, axis=-1, keepdims=True) + epsilon)
    return scaled * gain


def block_state(keys, value_rows, input_block, forget_block, scale):
    cumulative = jnp.cumsum(forget_block, axis=-1)
    total_log = cumulative[..., -1]
    log_weight = total_log[..., None] - cumulative + input_block
    peak_log = jnp.max(log_weight, axis=-1)
    weights = jnp.exp(log_weight - peak_log[..., None])
    key_float = keys.astype(jnp.float32) * scale
    value_weighted = value_rows.astype(jnp.float32) * weights[..., None]
    memory = jnp.einsum("...sv,...sk->...vk", value_weighted, key_float, precision=highest)
    return (memory, peak_log, total_log)


def merge_state(earlier, later):
    peak_log = jnp.maximum(later[2] + earlier[1], later[1])
    fade_earlier = jnp.exp(later[2] + earlier[1] - peak_log)
    fade_later = jnp.exp(later[1] - peak_log)
    memory = fade_earlier[..., None, None] * earlier[0] + fade_later[..., None, None] * later[0]
    return (memory, peak_log, earlier[2] + later[2])


def block_out(queries, keys, value_rows, input_block, forget_block, state, scale):
    cumulative = jnp.cumsum(forget_block, axis=-1)
    length = cumulative.shape[-1]
    causal = jnp.tril(jnp.ones((length, length), dtype=bool))
    within = jnp.where(
        causal,
        cumulative[..., :, None] - cumulative[..., None, :] + input_block[..., None, :],
        -jnp.inf,
    )
    carried = cumulative + state[1][..., None]
    highest_log = jnp.maximum(jnp.max(within, axis=-1), carried)
    weight_within = jnp.exp(within - highest_log[..., None])
    weight_carried = jnp.exp(carried - highest_log)
    raw_scores = (
        jnp.einsum("...td,...sd->...ts", queries, keys, preferred_element_type=jnp.float32) * scale
    )
    block_scores = raw_scores * weight_within
    numerator = jnp.einsum(
        "...ts,...sd->...td",
        block_scores.astype(jnp.bfloat16),
        value_rows,
        preferred_element_type=jnp.float32,
    )
    query_float = queries.astype(jnp.float32)
    return numerator + weight_carried[..., None] * jnp.einsum(
        "...vk,...tk->...tv", state[0], query_float, precision=highest
    )


def take_block(states, block_index):
    return tuple((member[block_index] for member in states))


def route_weights(group_logits, expert_logits, routes):
    members = expert_logits.shape[1] // group_logits.shape[1]
    chosen = jnp.take_along_axis(expert_logits, routes, axis=1)
    group_pick = jnp.take_along_axis(group_logits, routes // members, axis=1)
    return jax.nn.sigmoid(group_pick) * jax.nn.sigmoid(chosen - chosen[:, ::-1])


def shards(
    mixer_in,
    mixer_gain,
    query_weight,
    key_weight,
    value_weight,
    input_gate,
    forget_gate,
    head_gain,
    mixer_out_weight,
    expert_in,
    expert_gain,
    group_router,
    expert_router,
    routes,
    gate_experts,
    up_experts,
    down_experts,
):
    normed_a = rms_rows(mixer_in, mixer_gain).astype(jnp.bfloat16)
    queries = jnp.dot(normed_a, query_weight, preferred_element_type=jnp.float32).astype(
        jnp.bfloat16
    )
    keys = jnp.dot(normed_a, key_weight, preferred_element_type=jnp.float32).astype(jnp.bfloat16)
    value_rows = jnp.dot(normed_a, value_weight, preferred_element_type=jnp.float32).astype(
        jnp.bfloat16
    )
    row_count = normed_a.shape[0]
    head_local = input_gate.shape[0]
    width_local = queries.shape[1]
    head_size = width_local // head_local
    block_count = row_count // BLOCK
    scale = head_size ** (-0.5)

    def split_heads(matrix):
        return matrix.reshape(block_count, BLOCK, head_local, head_size).transpose(0, 2, 1, 3)

    def split_gates(gates):
        return gates.reshape(head_local, block_count, BLOCK).transpose(1, 0, 2)

    query_blocks = split_heads(queries)
    key_blocks = split_heads(keys)
    value_blocks = split_heads(value_rows)
    input_blocks = split_gates(input_gate)
    forget_blocks = split_gates(jax.nn.log_sigmoid(forget_gate))
    summaries = block_state(key_blocks, value_blocks, input_blocks, forget_blocks, scale)
    summary = take_block(summaries, 0)
    for block_index in range(1, block_count):
        summary = merge_state(summary, take_block(summaries, block_index))
    identity = (
        jnp.zeros_like(summary[0]),
        jnp.full_like(summary[1], floor_log),
        jnp.zeros_like(summary[2]),
    )
    current = prefix_by_axis(summary, EP, merge_state, identity)
    start_list = [current]
    for block_index in range(block_count - 1):
        current = merge_state(current, take_block(summaries, block_index))
        start_list.append(current)
    starts = tuple((jnp.stack([entry[member] for entry in start_list]) for member in range(3)))
    cells = block_out(
        query_blocks, key_blocks, value_blocks, input_blocks, forget_blocks, starts, scale
    )
    cells = cells.transpose(0, 2, 1, 3).reshape(row_count, head_local, head_size)
    gain_local = lax.dynamic_slice_in_dim(
        head_gain, lax.axis_index("tp") * width_local, width_local
    ).reshape(head_local, head_size)
    cell_rows = rms_rows(cells, gain_local).reshape(row_count, width_local).astype(jnp.bfloat16)
    tp_count = lax.axis_size("tp")
    out_weights = lax.all_gather(mixer_out_weight, "tp")
    cell_groups = lax.all_to_all(split_up(cell_rows, 0, tp_count), "tp", 0, 0, tiled=True)
    mixer_parts = jnp.einsum(
        "gtw,gwo->gto", cell_groups, out_weights, preferred_element_type=jnp.float32
    ).astype(jnp.bfloat16)
    mixer_out = jnp.sum(mixer_parts.astype(jnp.float32), axis=0).astype(jnp.bfloat16)
    normed_b = rms_rows(expert_in, expert_gain).astype(jnp.bfloat16)
    group_logits = jnp.dot(normed_b, group_router, preferred_element_type=jnp.float32)
    expert_logits = jnp.dot(normed_b, expert_router, preferred_element_type=jnp.float32)
    combine = route_weights(group_logits, expert_logits, routes)
    token_count = normed_b.shape[0]
    expert_total = expert_logits.shape[1]
    capacity = 4 * token_count // expert_total
    flat_routes = routes.reshape(-1)
    pair_total = flat_routes.shape[0]
    matches = (flat_routes[:, None] == jnp.arange(expert_total, dtype=jnp.int32)[None, :]).astype(
        jnp.int32
    )
    sequence_place = jnp.sum(jnp.cumsum(matches, axis=0) * matches, axis=1) - 1
    slot_index = flat_routes * capacity + sequence_place
    owner = (
        jnp.full((expert_total * capacity,), pair_total, jnp.int32)
        .at[slot_index]
        .set(jnp.arange(pair_total, dtype=jnp.int32))
    )
    share = normed_b.shape[1] // tp_count
    own_share = lax.dynamic_slice_in_dim(normed_b, lax.axis_index("tp") * share, share, axis=1)
    padded = jnp.concatenate([own_share, jnp.zeros((1, share), jnp.bfloat16)], axis=0)
    outgoing = padded[owner // 2].reshape(expert_total, capacity, share)
    gate_weight = gate_experts[0]
    up_weight = up_experts[0]
    down_weight = down_experts[0]
    down_parts = lax.all_to_all(split_up(down_weight, 1, tp_count), "tp", 0, 0, tiled=True)
    arrived = lax.all_to_all(outgoing, EP, split_axis=0, concat_axis=0, tiled=True)
    arrived = lax.all_gather(arrived.reshape(-1, share), "tp")
    gate_split = gate_weight.reshape(tp_count, share, -1)
    up_split = up_weight.reshape(tp_count, share, -1)
    gate_act = jnp.einsum("qsd,qdf->sf", arrived, gate_split, preferred_element_type=jnp.float32)
    up_act = jnp.einsum("qsd,qdf->sf", arrived, up_split, preferred_element_type=jnp.float32)
    hidden = (jax.nn.silu(gate_act) * up_act).astype(jnp.bfloat16)
    hidden = lax.all_gather(hidden, "tp")
    partial_rows = jnp.einsum(
        "gsf,gfo->gso", hidden, down_parts, preferred_element_type=jnp.float32
    ).astype(jnp.bfloat16)
    summed = jnp.sum(partial_rows.astype(jnp.float32), axis=0).astype(jnp.bfloat16)
    summed = summed.reshape(expert_total, capacity, share)
    returned = lax.all_to_all(summed, EP, split_axis=0, concat_axis=0, tiled=True)
    picked = jnp.take(returned.reshape(-1, returned.shape[2]), slot_index, axis=0).astype(
        jnp.float32
    )
    weighted = picked * combine.reshape(-1)[:, None]
    expert_out = jnp.sum(weighted.reshape(token_count, 2, weighted.shape[1]), axis=1).astype(
        jnp.bfloat16
    )
    return (mixer_out, expert_out)


def solution(mesh):
    split = Mesh(mesh.devices.reshape(8, 4, 2, mesh.shape["tp"]), ("ep_0", "ep_1", "ep_2", "tp"))
    placed = (
        P(EP, None),
        P(),
        P(None, "tp"),
        P(None, "tp"),
        P(None, "tp"),
        P("tp", EP),
        P("tp", EP),
        P(),
        P("tp", None),
        P(EP, None),
        P(),
        P(),
        P(),
        P(EP, None),
        P(EP, None, "tp"),
        P(EP, None, "tp"),
        P(EP, "tp", None),
    )
    return jax.shard_map(
        shards,
        mesh=split,
        in_specs=placed,
        out_specs=(P(EP_TP, None), P(EP, "tp")),
        check_vma=False,
    )
```

```python
import functools
from types import SimpleNamespace

import jax
import jax.numpy as jnp
from jax import lax
from jax.experimental import pallas as pl
from jax.experimental.pallas import tpu as pltpu
from jax.sharding import PartitionSpec as P

MESH = pl.DeviceIdType.MESH
F32 = jnp.float32
BF16 = jnp.bfloat16
BLOCK = 128
CORES = 2
NEAR = 2
EPSILON = 1e-06
FLOOR = -1e30
HIGHEST = lax.Precision.HIGHEST
STATE_ROWS = BLOCK + 16


def dot(a, b, dims=((1,), (0,)), precision=None):
    return lax.dot_general(a, b, (dims, ((), ())), precision=precision, preferred_element_type=F32)


def split(x):
    high = x.astype(BF16)
    return high, (x - high.astype(F32)).astype(BF16)


def visits(nz):
    order = []
    for d in range(2, nz // 2 + 1):
        order += [d] if 2 * d == nz else [d, -d]
    return order + ([1] if nz == 2 else [-1, 1]) + [0]


def merge(earlier, later):
    peak = jnp.maximum(later[2] + earlier[1], later[1])
    fade_earlier = jnp.exp(later[2] + earlier[1] - peak)
    fade_later = jnp.exp(later[1] - peak)
    return (fade_earlier * earlier[0] + fade_later * later[0], peak, earlier[2] + later[2])


def identity(depth=BLOCK):
    return (
        jnp.zeros((depth, BLOCK), F32),
        jnp.full((1, BLOCK), FLOOR, F32),
        jnp.zeros((1, BLOCK), F32),
    )


def load_state(ref, n):
    depth = ref.shape[1] - 16
    return ref[n, 0:depth, :], ref[n, depth : depth + 1, :], ref[n, depth + 8 : depth + 9, :]


def store_state(ref, n, state):
    depth = ref.shape[1] - 16
    ref[n, 0:depth, :] = state[0]
    ref[n, depth : depth + 8, :] = jnp.broadcast_to(state[1], (8, BLOCK))
    ref[n, depth + 8 : depth + 16, :] = jnp.broadcast_to(state[2], (8, BLOCK))


def chosen(pred, a, b):
    return tuple(jnp.where(pred, s, t) for s, t in zip(a, b))


def log_sigmoid(x):
    small = jnp.exp(-jnp.abs(x))
    whole = 1.0 + small
    direct = jnp.log(whole) + (small - (whole - 1.0)) / whole
    series = small * (
        1.0 - small * (0.5 - small * (1.0 / 3.0 - small * (0.25 - small * (0.2 - small / 6.0))))
    )
    return jnp.minimum(x, 0.0) - jnp.where(small < 1.0 / 64.0, series, direct)


def norm_rows(src, dst, gain, rows, step, base=0):
    def body(i, carry):
        at = pl.ds(pl.multiple_of(base + i * step, step), step)
        wide = src[at, :].astype(F32)
        scaled = wide * lax.rsqrt(jnp.mean(wide * wide, axis=-1, keepdims=True) + EPSILON)
        dst[at, :] = (scaled * gain[...]).astype(BF16)
        return carry

    lax.fori_loop(0, rows // step, body, 0)


def kernel(dims, *refs):
    nz, ny, nx = dims.nz, dims.ny, dims.nx
    r = SimpleNamespace(**dict(zip(dims.names, refs)))
    plane = ny * CORES
    n_ep = nz * plane
    tokens = r.x_b.shape[0]
    width = r.x_b.shape[1]
    share = width // nx
    slots = r.outg.shape[0]
    cap = slots // n_ep
    chunk = plane * cap
    half = chunk // 2
    hid_w = r.gate.shape[1]
    heads = r.i_gate.shape[0]
    rows_a = r.x_a.shape[0]
    blocks = rows_a // BLOCK
    scale = BLOCK ** (-0.5)

    ep = lax.axis_index("ep")
    x = lax.axis_index("tp")
    z = lax.div(ep, plane)
    y = lax.div(lax.rem(ep, plane), CORES)
    c = lax.rem(ep, CORES)
    order = visits(nz)
    wide_from = nz - dims.near

    def offset(j):
        total = 0
        for k, d in enumerate(order):
            total = jnp.where(j == k, d, total)
        return total

    right = lax.rem(x + 1, nx)
    left = lax.rem(x + nx - 1, nx)
    mate = ep + 1 - 2 * c

    def rows(at, count, unit):
        return pl.ds(pl.multiple_of(at, unit), count)

    def remote(src, dst, send, recv, to_ep, to_x):
        return pltpu.make_async_remote_copy(
            src_ref=src,
            dst_ref=dst,
            send_sem=send,
            recv_sem=recv,
            device_id=(to_ep, to_x),
            device_id_type=MESH,
        )

    def settle(view, sem):
        pltpu.make_async_copy(view, view, sem).wait()

    barrier = pltpu.get_barrier_semaphore()

    def greet(k, carry):
        to = lax.rem(ep + k, n_ep)
        pl.semaphore_signal(barrier, inc=1, device_id=(to, x), device_id_type=MESH)
        return carry

    lax.fori_loop(1, n_ep, greet, 0)
    for k in range(1, nx):
        to = lax.rem(x + k, nx)
        pl.semaphore_signal(barrier, inc=1, device_id=(ep, to), device_id_type=MESH)

    down_at = r.down_h.at[:, rows(x * share, share, 128)]
    loads = SimpleNamespace()
    for n, (name, pair) in enumerate(
        dict(
            x_b=(r.x_b, r.xb),
            x_a=(r.x_a, r.xa),
            wq=(r.wq_h, r.wq),
            wk=(r.wk_h, r.wk),
            wv=(r.wv_h, r.wv),
            gate=(r.gate_h, r.gate),
            up=(r.up_h, r.up),
            group=(r.group_h, r.group),
            expert=(r.expert_h, r.expert),
            down=(down_at, r.down.at[x]),
            wout=(r.wout_h, r.wout.at[x]),
        ).items()
    ):
        load = pltpu.make_async_copy(*pair, r.load_s.at[n])
        setattr(loads, name, load)
    loads.x_b.start()

    route_rows = r.routes[...]
    experts_iota = lax.broadcasted_iota(jnp.int32, (n_ep, tokens), 0)
    hit0 = experts_iota == route_rows[0:1, :]
    hit1 = experts_iota == route_rows[1:2, :]
    named = jnp.where(hit0, 1.0, 0.0) + jnp.where(hit1, 1.0, 0.0)
    before = jnp.where(
        lax.broadcasted_iota(jnp.int32, (tokens, tokens), 0)
        < lax.broadcasted_iota(jnp.int32, (tokens, tokens), 1),
        1.0,
        0.0,
    ).astype(BF16)
    counts = dot(named.astype(BF16), before)
    place0 = jnp.sum(jnp.where(hit0, counts, 0.0), axis=0, keepdims=True)
    place1 = jnp.sum(jnp.where(hit1, counts, 0.0), axis=0, keepdims=True)
    route0 = route_rows[0:1, :].astype(F32)
    route1 = route_rows[1:2, :].astype(F32)
    slot0 = route0 * cap + place0
    slot1 = route1 * cap + place1
    flip = r.flip
    flip[...] = jnp.zeros_like(flip)
    flip[0:1, :] = route0
    flip[1:2, :] = route1
    flip[2:3, :] = slot0
    flip[3:4, :] = slot1
    r.cols[...] = jnp.transpose(flip[...])

    loads.x_b.wait()
    for load in list(vars(loads).values())[1:]:
        load.start()
    norm_rows(r.xb, r.nb, r.gain_b, tokens, min(32, tokens))

    def packed(j, wide):
        z_to = lax.rem(z - offset(j) + nz, nz)
        base = z_to * chunk
        place = (lax.broadcasted_iota(jnp.int32, (chunk, tokens), 0) + base).astype(F32)
        taken = jnp.where(place == flip[2:3, :], 1.0, 0.0) + jnp.where(
            place == flip[3:4, :], 1.0, 0.0
        )
        taken = taken.astype(BF16)
        if wide:
            for q in range(nx):
                part = r.nb[:, q * share : (q + 1) * share]
                r.near[j - wide_from, q, :, :] = dot(taken, part).astype(BF16)
        else:
            own = r.nb[:, rows(x * share, share, 128)]
            r.outg[rows(base, chunk, chunk), :] = dot(taken, own).astype(BF16)

    def pack_near(j, carry):
        packed(j, True)
        return carry

    def pack_far(j, carry):
        packed(j, False)
        return carry

    lax.fori_loop(0, wide_from, pack_far, 0)
    lax.fori_loop(wide_from, nz, pack_near, 0)

    pl.semaphore_wait(barrier, n_ep - 1 + nx - 1)

    far = lax.rem(x + 2, nx)
    fold = hid_w // 2
    for k, to in enumerate((right, left)):
        remote(
            r.down_h.at[:, rows(to * share, share, 128)],
            r.down.at[x],
            r.down_ss.at[k],
            r.down_rs.at[x],
            ep,
            to,
        ).start()
    for k, to in enumerate((right, left)):
        remote(
            r.down_h.at[k * fold : (k + 1) * fold, rows(far * share, share, 128)],
            r.relay.at[k],
            r.down_ss.at[2 + k],
            r.relay_rs.at[k],
            ep,
            to,
        ).start()

    def pass_down():
        for k, (source_x, to) in enumerate(((left, right), (right, left))):
            settle(r.relay.at[k], r.relay_rs.at[k])
            remote(
                r.relay.at[k],
                r.down.at[source_x, k * fold : (k + 1) * fold, :],
                r.down_ss.at[4 + k],
                r.far_rs.at[k],
                ep,
                to,
            ).start()

    def posted(j, wide):
        z_to = lax.rem(z - offset(j) + nz, nz)

        def post(k, inner):
            to = z_to * plane + k

            @pl.when(to != ep)
            def _():
                if wide:
                    src = r.near.at[j - wide_from, :, rows(k * cap, cap, cap), :]
                    dst = r.tok.at[:, rows(ep * cap, cap, cap), :]
                else:
                    src = r.outg.at[rows(to * cap, cap, cap), :]
                    dst = r.tok.at[x, rows(ep * cap, cap, cap), :]
                remote(src, dst, r.disp_ss.at[z_to], r.disp_rs.at[z], to, x).start()

            return inner

        lax.fori_loop(0, plane, post, 0)

    def post_near(j, carry):
        posted(j, True)
        return carry

    def post_far(j, carry):
        posted(j, False)
        return carry

    lax.fori_loop(0, wide_from, post_far, 0)
    lax.fori_loop(wide_from, nz, post_near, 0)
    own_rows = rows(ep * cap, cap, cap)
    own_place = rows(lax.rem(ep, plane) * cap, cap, cap)
    kept = pltpu.make_async_copy(
        r.near.at[dims.near - 1, :, own_place, :], r.tok.at[:, own_rows, :], r.kept_s.at[0]
    )
    kept.start()

    def ring_of(me, count, device):
        after, ahead = lax.rem(me + 1, count), lax.rem(me + count - 1, count)
        return SimpleNamespace(
            me=me,
            right=after,
            left=ahead,
            far=lax.rem(me + 2, count),
            to_right=device(after),
            to_left=device(ahead),
        )

    over_x = ring_of(x, nx, lambda to: (ep, to))
    over_y = ring_of(y, ny, lambda to: (z * plane + to * CORES + c, x))

    def ring_start(ring, view, src, ss, rs, j):
        remote(src, view(ring.me), ss.at[0, j], rs.at[0, j], *ring.to_right).start()
        remote(src, view(ring.me), ss.at[1, j], rs.at[1, j], *ring.to_left).start()

    def ring_forward(ring, view, low, high, ss, rs, j):
        settle(view(ring.left), rs.at[0, j])
        part = low(ring.left)
        remote(part, part, ss.at[2, j], rs.at[2, j], *ring.to_right).start()
        settle(view(ring.right), rs.at[1, j])
        part = high(ring.right)
        remote(part, part, ss.at[3, j], rs.at[3, j], *ring.to_left).start()

    def ring_finish(ring, low, high, rs, j):
        settle(low(ring.far), rs.at[2, j])
        settle(high(ring.far), rs.at[3, j])

    def ring_sent(ring, view, low, high, ss, j):
        settle(view(ring.me), ss.at[0, j])
        settle(view(ring.me), ss.at[1, j])
        settle(low(ring.left), ss.at[2, j])
        settle(high(ring.right), ss.at[3, j])

    def source(j):
        return lax.rem(z + offset(j) + nz, nz)

    def tok_views(j):
        base = source(j) * chunk
        return (
            lambda q: r.tok.at[q, rows(base, chunk, chunk), :],
            lambda q: r.tok.at[q, rows(base, half, half), :],
            lambda q: r.tok.at[q, rows(base + half, half, half), :],
        )

    def hid_views(j):
        base = source(j) * chunk
        return (
            lambda q: r.hid.at[q, rows(base, chunk, chunk), :],
            lambda q: r.hid.at[q, rows(base, half, half), :],
            lambda q: r.hid.at[q, rows(base + half, half, half), :],
        )

    out_half = r.wout.shape[1] // CORES
    out_part = out_half // ny

    def wout_views(q=None):
        def cut(base, count):
            def view(n):
                at, place = (n, y) if q is None else (q, n)
                return r.wout.at[at, rows(c * out_half + place * out_part + base, count, 16), :]

            return view

        return cut(0, out_part), cut(0, out_part // 2), cut(out_part // 2, out_part // 2)

    others = [lax.rem(x + k, nx) for k in range(1, nx)]

    def wout_half(q):
        return r.wout.at[q, rows(c * out_half, out_half, out_half), :]

    def take_rows(j):
        view, low, high = tok_views(j)
        settle(view(x), r.disp_rs.at[source(j)])
        ring_start(over_x, view, view(x), r.tok_ss, r.tok_rs, j)

    def expand(j):
        view, low, high = tok_views(j)
        at = rows(source(j) * chunk, chunk, chunk)

        @pl.when(j == nz - 1)
        def _():
            settle(r.near.at[0, :, rows(0, chunk - cap, cap), :], r.disp_rs.at[z])
            kept.wait()

        @pl.when(jnp.logical_and(j >= wide_from, j < nz - 1))
        def _():
            settle(r.tok.at[:, at, :], r.disp_rs.at[source(j)])

        @pl.when(j < wide_from)
        def _():
            ring_finish(over_x, low, high, r.tok_rs, j)

        gated = jnp.zeros((chunk, hid_w), F32)
        upped = jnp.zeros((chunk, hid_w), F32)
        for q in range(nx):
            part = r.tok[q, at, :]
            gated += dot(part, r.gate[q * share : (q + 1) * share, :])
            upped += dot(part, r.up[q * share : (q + 1) * share, :])
        r.hid[x, at, :] = (gated * jax.nn.sigmoid(gated) * upped).astype(BF16)
        hview = hid_views(j)[0]
        ring_start(over_x, hview, hview(x), r.hid_ss, r.hid_rs, j)

    def contract(j):
        view, low, high = hid_views(j)
        ring_finish(over_x, low, high, r.hid_rs, j)
        z_to = source(j)
        at = rows(z_to * chunk, chunk, chunk)
        total = jnp.zeros((chunk, share), F32)
        for q in range(nx):
            total += dot(r.hid[q, at, :], r.down[q]).astype(BF16).astype(F32)
        r.res[at, :] = total.astype(BF16)

        def post(k, inner):
            to = z_to * plane + k

            @pl.when(to != ep)
            def _():
                remote(
                    r.res.at[rows(to * cap, cap, cap), :],
                    r.ret.at[rows(ep * cap, cap, cap), :],
                    r.ret_ss.at[z_to],
                    r.ret_rs.at[z],
                    to,
                    x,
                ).start()

            return inner

        lax.fori_loop(0, plane, post, 0)

        @pl.when(j == nz - 1)
        def _():
            pltpu.make_async_copy(
                r.res.at[own_rows, :], r.ret.at[own_rows, :], r.kept_s.at[1]
            ).start()

    def gather_up(j):
        z_from = lax.rem(z - offset(j) + nz, nz)
        base = z_from * chunk
        at = rows(base, chunk, chunk)

        @pl.when(j == 0)
        def _():
            r.acc[...] = jnp.zeros_like(r.acc)

        @pl.when(j == nz - 1)
        def _():
            settle(r.res.at[rows(0, chunk - cap, cap), :], r.ret_rs.at[z])
            settle(r.res.at[rows(0, cap, cap), :], r.kept_s.at[1])

        @pl.when(j < nz - 1)
        def _():
            settle(r.ret.at[at, :], r.ret_rs.at[z_from])

        lane = (lax.broadcasted_iota(jnp.int32, (tokens, chunk), 1) + base).astype(F32)
        back = r.ret[at, :]
        for k in range(2):
            picks = jnp.where(lane == r.cols[:, 2 + k : 3 + k], 1.0, 0.0).astype(BF16)
            r.acc[...] += r.comb[:, k : k + 1] * dot(picks, back)

    def weights():
        loads.group.wait()
        loads.expert.wait()
        normed = r.nb[...]
        group_logits = dot(normed, r.group[...], ((1,), (1,)))
        expert_logits = dot(normed, r.expert[...], ((1,), (1,)))
        members = expert_logits.shape[1] // group_logits.shape[1]
        groups_iota = lax.broadcasted_iota(jnp.int32, group_logits.shape, 1)
        lanes_iota = lax.broadcasted_iota(jnp.int32, expert_logits.shape, 1)
        picked, grouped = [], []
        for k in range(2):
            route = r.cols[:, k : k + 1].astype(jnp.int32)
            picked.append(
                jnp.sum(jnp.where(lanes_iota == route, expert_logits, 0.0), axis=1, keepdims=True)
            )
            first = route - groups_iota * members
            inside = jnp.logical_and(first >= 0, first < members)
            grouped.append(jnp.sum(jnp.where(inside, group_logits, 0.0), axis=1, keepdims=True))
        for k in range(2):
            r.comb[:, k : k + 1] = jax.nn.sigmoid(grouped[k]) * jax.nn.sigmoid(
                picked[k] - picked[1 - k]
            )

    def project(first, last):
        if first == 0:
            loads.x_a.wait()
            loads.wq.wait()
            loads.wk.wait()
            loads.wv.wait()

        def body(b, carry):
            at = rows(b * BLOCK, BLOCK, BLOCK)
            norm_rows(r.xa, r.na, r.gain_a, BLOCK, 32, b * BLOCK)
            normed = r.na[at, :]
            for weight, to in ((r.wq, r.q), (r.wk, r.k), (r.wv, r.v)):
                to[at, :] = dot(normed, weight[...]).astype(BF16)
            return carry

        lax.fori_loop(first, last, body, 0)

    def pieces(n):
        h, b = n // blocks, n % blocks
        at = (slice(b * BLOCK, (b + 1) * BLOCK), slice(h * BLOCK, (h + 1) * BLOCK))
        return r.q[at], r.k[at], r.v[at]

    def summarize():
        logs = log_sigmoid(r.f_gate[...])
        inputs = r.i_gate[...]
        gates = r.gates
        for n in range(heads * blocks):
            h, b = n // blocks, n % blocks
            lanes = slice(b * BLOCK, (b + 1) * BLOCK)
            gates[n : n + 1, :] = logs[h : h + 1, lanes]
            gates[16 + n : 17 + n, :] = inputs[h : h + 1, lanes]
        upto = jnp.where(
            lax.broadcasted_iota(jnp.int32, (BLOCK, BLOCK), 0)
            <= lax.broadcasted_iota(jnp.int32, (BLOCK, BLOCK), 1),
            1.0,
            0.0,
        )
        count = heads * blocks
        sums = dot(gates[0:count, :], upto, precision=HIGHEST)
        totals = sums[:, BLOCK - 1 : BLOCK]
        log_weight = totals - sums + gates[16 : 16 + count, :]
        peaks = jnp.max(log_weight, axis=1, keepdims=True)
        turn = r.turn
        turn[...] = jnp.zeros_like(turn)
        turn[0:count, :] = sums
        turn[count : 2 * count, :] = jnp.exp(log_weight - peaks)
        turned = jnp.transpose(turn[...])
        r.turned[...] = turned
        for h in range(heads):
            summary = None
            for b in range(blocks):
                n = h * blocks + b
                _, keys, values = pieces(n)
                high, low = split(values.astype(F32) * turned[:, count + n : count + n + 1])
                memory = scale * (dot(keys, high, ((0,), (0,))) + dot(keys, low, ((0,), (0,))))
                state = (
                    memory,
                    jnp.broadcast_to(peaks[n : n + 1, :], (1, BLOCK)),
                    jnp.broadcast_to(totals[n : n + 1, :], (1, BLOCK)),
                )
                store_state(r.sums, n, state)
                summary = state if summary is None else merge(summary, state)
            store_state(r.own, h, summary)
        remote(r.own, r.other, r.mate_ss.at[0], r.mate_rs.at[0], mate, x).start()

    def chip_level():
        settle(r.other, r.mate_rs.at[0])
        mine, theirs = load_state(r.own, c), load_state(r.other, c)
        first = c == 0
        store_state(
            r.y_in, y, merge(chosen(first, mine, theirs), chosen(first, theirs, mine))
        )
        for k in range(1, ny):
            y_to = lax.rem(y + k, ny)
            remote(
                r.y_in.at[y],
                r.y_in.at[y],
                r.y_ss.at[k],
                r.y_rs.at[y],
                z * plane + y_to * CORES + c,
                x,
            ).start()

    def run_up(ref, count, place, run):
        depth = run.shape[1] - 16
        store_state(run, 0, identity(depth))
        store_state(run, 1, identity(depth))

        def body(k, carry):
            after = merge(load_state(run, 1), load_state(ref, k))

            store_state(run, 1, after)

            @pl.when(k + 1 == place)
            def _():
                store_state(run, 0, after)

            return carry

        lax.fori_loop(0, count, body, 0)

    def plane_level():
        for k in range(1, ny):
            y_from = lax.rem(y + k, ny)
            settle(r.y_in.at[y_from], r.y_rs.at[y_from])
        run_up(r.y_in, ny, y, r.y_run)
        _, peak, total = load_state(r.y_run, 1)
        part = r.z_in.shape[1] - 16
        store_state(r.z_in, z, (r.y_run[1, rows(y * part, part, part), :], peak, total))
        for k in range(1, nz):
            z_to = lax.rem(z + k, nz)
            remote(
                r.z_in.at[z],
                r.z_in.at[z],
                r.z_ss.at[k],
                r.z_rs.at[z],
                z_to * plane + y * CORES + c,
                x,
            ).start()

    def line_level():
        for k in range(1, nz):
            z_from = lax.rem(z + k, nz)
            settle(r.z_in.at[z_from], r.z_rs.at[z_from])
        run_up(r.z_in, nz, z, r.z_run)
        store_state(r.line, y, load_state(r.z_run, 0))
        for k in range(1, ny):
            y_to = lax.rem(y + k, ny)
            remote(
                r.line.at[y],
                r.line.at[y],
                r.line_ss.at[k],
                r.line_rs.at[y],
                z * plane + y_to * CORES + c,
                x,
            ).start()

    def start_level():
        for k in range(1, ny):
            y_from = lax.rem(y + k, ny)
            settle(r.line.at[y_from], r.line_rs.at[y_from])
        parts = [load_state(r.line, k) for k in range(ny)]
        memory = jnp.concatenate([part[0] for part in parts], axis=0)
        store_state(r.start, c, merge((memory, *parts[0][1:]), load_state(r.y_run, 0)))
        remote(
            r.start.at[c],
            r.start.at[c],
            r.mate_ss.at[1],
            r.mate_rs.at[1],
            mate,
            x,
        ).start()

    def attend(first, last):
        if first == 0:
            settle(r.start.at[1 - c], r.mate_rs.at[1])
        count = heads * blocks
        turned = r.turned
        gates = r.gates
        states = []
        for h in range(heads):
            if first == 0:
                later = chosen(c == 1, load_state(r.other, h), identity())
                states.append(merge(load_state(r.start, h), later))
            else:
                states.append(load_state(r.current, h))
        causal = lax.broadcasted_iota(jnp.int32, (BLOCK, BLOCK), 0) >= lax.broadcasted_iota(
            jnp.int32, (BLOCK, BLOCK), 1
        )
        for b in range(first, last):
            for h in range(heads):
                n = h * blocks + b
                queries, keys, values = pieces(n)
                memory, peak, _ = states[h]
                column = turned[:, n : n + 1]
                within = column - r.turn[n : n + 1, :] + gates[16 + n : 17 + n, :]
                within = jnp.where(causal, within, FLOOR)
                carried = column + peak[:, 0:1]
                top = jnp.maximum(jnp.max(within, axis=1, keepdims=True), carried)
                raw = dot(queries, keys, ((1,), (1,))) * scale
                scores = (raw * jnp.exp(within - top)).astype(BF16)
                high, low = split(memory)
                recalled = dot(queries, high) + dot(queries, low)
                cells = dot(scores, values) + jnp.exp(carried - top) * recalled
                square = jnp.mean(cells * cells, axis=1, keepdims=True)
                gain = r.gain_h[pl.ds(x * heads + h, 1), :]
                r.cell[b, :, h * BLOCK : (h + 1) * BLOCK] = (
                    cells * lax.rsqrt(square + EPSILON) * gain
                ).astype(BF16)
                if b + 1 < blocks:
                    states[h] = merge(states[h], load_state(r.sums, n))
        if last < blocks:
            for h in range(heads):
                store_state(r.current, h, states[h])
            return
        for k in range(1, nx):
            to = lax.rem(x + k, nx)
            remote(
                r.cell.at[to],
                r.cells.at[x],
                r.cell_ss.at[k],
                r.cell_rs.at[x],
                ep,
                to,
            ).start()
        r.cells[x] = r.cell[x]

    def mix_out():
        for k in range(1, nx):
            q = lax.rem(x + k, nx)
            settle(r.cells.at[q], r.cell_rs.at[q])
            other_half = rows((1 - c) * out_half, out_half, out_half)
            settle(r.wout.at[q, other_half, :], r.wm_rs.at[q])
        loads.wout.wait()
        step = r.mixed.shape[1] // 4
        for n in range(4):
            lanes = slice(n * step, (n + 1) * step)
            total = jnp.zeros((BLOCK, step), F32)
            for g in range(nx):
                total += dot(r.cells[g], r.wout[g, :, lanes]).astype(BF16).astype(F32)
            r.mixed[:, lanes] = total.astype(BF16)
        pltpu.make_async_copy(r.mixed, r.out_a, r.out_s.at[0]).start()

    when, lag = dims.when, dims.lag

    def at_step(number, job):
        @pl.when(jnp.logical_and(number >= 0, number < nz))
        def _():
            job(number)

    def far_only(job):
        def run(j):
            @pl.when(j < wide_from)
            def _():
                job(j)

        return run

    def forward_rows(j):
        ring_forward(over_x, *tok_views(j), r.tok_ss, r.tok_rs, j)

    def forward_hidden(j):
        ring_forward(over_x, *hid_views(j), r.hid_ss, r.hid_rs, j)

    def down_arrived():
        loads.down.wait()
        for k, source_x in enumerate((left, right)):
            settle(r.down.at[source_x], r.down_rs.at[source_x])
            settle(r.relay.at[k], r.far_rs.at[k])

    def experts_arrived():
        loads.gate.wait()
        loads.up.wait()

    def wout_start():
        own = r.wout_h.at[rows(c * out_half + y * out_part, out_part, 16), :]
        ring_start(over_x, wout_views()[0], own, r.w_ss, r.w_rs, 0)

    def wout_forward():
        ring_forward(over_x, *wout_views(), r.w_ss, r.w_rs, 0)

    def wout_turn():
        ring_finish(over_x, *wout_views()[1:], r.w_rs, 0)
        for k, q in enumerate(others):
            view = wout_views(q)[0]
            ring_start(over_y, view, view(y), r.wy_ss, r.wy_rs, k)

    def wout_pass():
        for k, q in enumerate(others):
            ring_forward(over_y, *wout_views(q), r.wy_ss, r.wy_rs, k)

    def wout_spread():
        for k, q in enumerate(others):
            ring_finish(over_y, *wout_views(q)[1:], r.wy_rs, k)
            half = wout_half(q)
            remote(half, half, r.wm_ss.at[k], r.wm_rs.at[q], mate, x).start()

    first_jobs = ((lag.expand, experts_arrived), (lag.contract, down_arrived))
    jobs = (
        (when.pass_down, pass_down),
        (when.wout_start, wout_start),
        (when.chip, chip_level),
        (when.plane, plane_level),
        (when.wout_forward, wout_forward),
        (when.line, line_level),
        (when.start, start_level),
        (when.weights, weights),
        (when.attend, functools.partial(attend, 0, blocks // 2)),
        (when.attend + 1, functools.partial(attend, blocks // 2, blocks)),
        (when.wout_turn, wout_turn),
        (when.wout_pass, wout_pass),
        (when.wout_spread, wout_spread),
        (when.mix, mix_out),
    )
    project(0, blocks)
    summarize()

    def step(i, carry):
        at_step(i - lag.take, far_only(take_rows))
        at_step(i - lag.forward, far_only(forward_rows))
        for place, job in first_jobs:
            pl.when(i == place)(job)
        at_step(i - lag.expand, expand)
        at_step(i - lag.hidden, forward_hidden)
        at_step(i - lag.contract, contract)
        at_step(i - lag.gather, gather_up)
        for place, job in jobs:
            pl.when(i == place)(job)
        return carry

    lax.fori_loop(0, max(nz + lag.gather, when.mix + 1), step, 0)

    r.mixed_b[...] = r.acc[...].astype(BF16)
    last = pltpu.make_async_copy(r.mixed_b, r.out_b, r.out_s.at[1])
    last.start()

    def sent(j, carry):
        z_to = lax.rem(z - offset(j) + nz, nz)
        ring_sent(over_x, *hid_views(j), r.hid_ss, j)

        @pl.when(j == nz - 1)
        def _():
            settle(r.near.at[0, :, rows(0, chunk - cap, cap), :], r.disp_ss.at[z])
            settle(r.res.at[rows(0, chunk - cap, cap), :], r.ret_ss.at[z])

        @pl.when(j < nz - 1)
        def _():
            settle(r.res.at[rows(0, chunk, chunk), :], r.ret_ss.at[z_to])

        @pl.when(jnp.logical_and(j >= wide_from, j < nz - 1))
        def _():
            settle(r.near.at[0], r.disp_ss.at[z_to])

        @pl.when(j < wide_from)
        def _():
            settle(r.outg.at[rows(0, chunk, chunk), :], r.disp_ss.at[z_to])
            ring_sent(over_x, *tok_views(j), r.tok_ss, j)

        return carry

    lax.fori_loop(0, nz, sent, 0)
    ring_sent(over_x, *wout_views(), r.w_ss, 0)
    for k, q in enumerate(others):
        ring_sent(over_y, *wout_views(q), r.wy_ss, k)
        settle(wout_half(q), r.wm_ss.at[k])
        settle(r.cell.at[x], r.cell_ss.at[k + 1])
    for k in range(2):
        settle(r.down.at[x], r.down_ss.at[k])
        settle(r.relay.at[0], r.down_ss.at[k + 2])
        settle(r.relay.at[0], r.down_ss.at[k + 4])
    for k in range(1, ny):
        settle(r.y_in.at[y], r.y_ss.at[k])
        settle(r.line.at[y], r.line_ss.at[k])
    for k in range(1, nz):
        settle(r.z_in.at[z], r.z_ss.at[k])
    settle(r.own, r.mate_ss.at[0])
    settle(r.start.at[c], r.mate_ss.at[1])
    settle(r.mixed, r.out_s.at[0])
    last.wait()


def solution(mesh, shape=(8, 4)):
    nz, ny = shape
    nx = mesh.shape["tp"]
    n_ep = mesh.shape["ep"]

    def shards(
        mixer_in,
        mixer_gain,
        query_weight,
        key_weight,
        value_weight,
        input_gate,
        forget_gate,
        head_gain,
        mixer_out_weight,
        expert_in,
        expert_gain,
        group_router,
        expert_router,
        routes,
        gate_experts,
        up_experts,
        down_experts,
    ):
        rows_a, width = mixer_in.shape
        near = min(NEAR, nz - 1)
        tokens = expert_in.shape[0]
        share = width // nx
        cap = 4 * tokens // n_ep
        slots = n_ep * cap
        heads = input_gate.shape[0]
        blocks = rows_a // BLOCK
        qkv = query_weight.shape[1]
        hid_w = gate_experts.shape[2]
        vmem = pl.BlockSpec(memory_space=pltpu.VMEM)
        hbm = pl.BlockSpec(memory_space=pl.ANY)
        inputs = dict(
            x_a=(mixer_in, hbm),
            gain_a=(mixer_gain.reshape(1, -1), vmem),
            wq_h=(query_weight, hbm),
            wk_h=(key_weight, hbm),
            wv_h=(value_weight, hbm),
            i_gate=(input_gate, vmem),
            f_gate=(forget_gate, vmem),
            gain_h=(head_gain.reshape(-1, BLOCK), vmem),
            wout_h=(mixer_out_weight, hbm),
            x_b=(expert_in, hbm),
            gain_b=(expert_gain.reshape(1, -1), vmem),
            group_h=(group_router.T, hbm),
            expert_h=(expert_router.T, hbm),
            routes=(routes.T, vmem),
            gate_h=(gate_experts[0], hbm),
            up_h=(up_experts[0], hbm),
            down_h=(down_experts[0], hbm),
        )
        state = (STATE_ROWS, BLOCK)
        part = (BLOCK // ny + 16, BLOCK)
        dma = pltpu.SemaphoreType.DMA
        scratch = dict(
            xa=pltpu.VMEM((rows_a, width), BF16),
            xb=pltpu.VMEM((tokens, width), BF16),
            wq=pltpu.VMEM(query_weight.shape, BF16),
            wk=pltpu.VMEM(query_weight.shape, BF16),
            wv=pltpu.VMEM(query_weight.shape, BF16),
            gate=pltpu.VMEM((width, hid_w), BF16),
            up=pltpu.VMEM((width, hid_w), BF16),
            group=pltpu.VMEM(group_router.shape[::-1], BF16),
            expert=pltpu.VMEM(expert_router.shape[::-1], BF16),
            down=pltpu.VMEM((nx, hid_w, share), BF16),
            relay=pltpu.VMEM((2, hid_w // 2, share), BF16),
            wout=pltpu.VMEM((nx, qkv, mixer_out_weight.shape[1]), BF16),
            flip=pltpu.VMEM((128, tokens), F32),
            cols=pltpu.VMEM((tokens, 128), F32),
            nb=pltpu.VMEM((tokens, width), BF16),
            outg=pltpu.VMEM((slots, share), BF16),
            near=pltpu.VMEM((near, nx, slots // nz, share), BF16),
            tok=pltpu.VMEM((nx, slots, share), BF16),
            hid=pltpu.VMEM((nx, slots, hid_w), BF16),
            res=pltpu.VMEM((slots, share), BF16),
            ret=pltpu.VMEM((slots, share), BF16),
            comb=pltpu.VMEM((tokens, 128), F32),
            acc=pltpu.VMEM((tokens, share), F32),
            mixed_b=pltpu.VMEM((tokens, share), BF16),
            na=pltpu.VMEM((rows_a, width), BF16),
            q=pltpu.VMEM((rows_a, qkv), BF16),
            k=pltpu.VMEM((rows_a, qkv), BF16),
            v=pltpu.VMEM((rows_a, qkv), BF16),
            gates=pltpu.VMEM((32, BLOCK), F32),
            turn=pltpu.VMEM((BLOCK, BLOCK), F32),
            turned=pltpu.VMEM((BLOCK, BLOCK), F32),
            sums=pltpu.VMEM((heads * blocks, *state), F32),
            own=pltpu.VMEM((heads, *state), F32),
            other=pltpu.VMEM((heads, *state), F32),
            start=pltpu.VMEM((heads, *state), F32),
            current=pltpu.VMEM((heads, *state), F32),
            y_in=pltpu.VMEM((ny, *state), F32),
            y_run=pltpu.VMEM((2, *state), F32),
            z_in=pltpu.VMEM((nz, *part), F32),
            z_run=pltpu.VMEM((2, *part), F32),
            line=pltpu.VMEM((ny, *part), F32),
            cell=pltpu.VMEM((nx, BLOCK, qkv), BF16),
            cells=pltpu.VMEM((nx, BLOCK, qkv), BF16),
            mixed=pltpu.VMEM((BLOCK, width), BF16),
            load_s=dma((11,)),
            kept_s=dma((2,)),
            out_s=dma((2,)),
            down_ss=dma((6,)),
            relay_rs=dma((2,)),
            far_rs=dma((2,)),
            down_rs=dma((nx,)),
            disp_ss=dma((nz,)),
            disp_rs=dma((nz,)),
            tok_ss=dma((4, nz)),
            tok_rs=dma((4, nz)),
            hid_ss=dma((4, nz)),
            hid_rs=dma((4, nz)),
            ret_ss=dma((nz,)),
            ret_rs=dma((nz,)),
            w_ss=dma((4, 1)),
            w_rs=dma((4, 1)),
            wy_ss=dma((4, nx - 1)),
            wy_rs=dma((4, nx - 1)),
            wm_ss=dma((nx,)),
            wm_rs=dma((nx,)),
            mate_ss=dma((2,)),
            mate_rs=dma((2,)),
            y_ss=dma((ny,)),
            y_rs=dma((ny,)),
            line_ss=dma((ny,)),
            line_rs=dma((ny,)),
            z_ss=dma((nz,)),
            z_rs=dma((nz,)),
            cell_ss=dma((nx,)),
            cell_rs=dma((nx,)),
        )
        names = [*inputs, "out_a", "out_b", *scratch]
        when = SimpleNamespace(
            chip=0,
            plane=2,
            weights=3,
            line=6,
            start=7,
            attend=8,
            pass_down=1,
            wout_start=1,
            wout_forward=3,
            wout_turn=4,
            wout_pass=6,
            wout_spread=9,
            mix=12,
        )
        lag = SimpleNamespace(take=0, forward=1, expand=2, hidden=3, contract=4, gather=6)
        dims = SimpleNamespace(nz=nz, ny=ny, nx=nx, near=near, names=names, when=when, lag=lag)
        return pl.pallas_call(
            functools.partial(kernel, dims),
            out_shape=(
                jax.ShapeDtypeStruct((rows_a // nx, width), BF16),
                jax.ShapeDtypeStruct((tokens, share), BF16),
            ),
            in_specs=[spec for _, spec in inputs.values()],
            out_specs=(hbm, hbm),
            scratch_shapes=list(scratch.values()),
            compiler_params=pltpu.CompilerParams(
                collective_id=0, has_side_effects=True, vmem_limit_bytes=60 * 1024 * 1024
            ),
            name="mixer_and_experts",
        )(*[value for value, _ in inputs.values()])

    placed = (
        P("ep", None),
        P(),
        P(None, "tp"),
        P(None, "tp"),
        P(None, "tp"),
        P("tp", "ep"),
        P("tp", "ep"),
        P(),
        P("tp", None),
        P("ep", None),
        P(),
        P(),
        P(),
        P("ep", None),
        P("ep", None, "tp"),
        P("ep", None, "tp"),
        P("ep", "tp", None),
    )
    return jax.shard_map(
        shards,
        mesh=mesh,
        in_specs=placed,
        out_specs=(P(("ep", "tp"), None), P("ep", "tp")),
        check_vma=False,
    )
```

```python
import functools
from types import SimpleNamespace

import jax
import jax.numpy as jnp
from jax import lax
from jax.experimental import pallas as pl
from jax.experimental.pallas import tpu as pltpu
from jax.sharding import PartitionSpec as P

MESH = pl.DeviceIdType.MESH
F32 = jnp.float32
BF16 = jnp.bfloat16
BLOCK = 128
CORES = 2
NEAR = 3
EPSILON = 1e-06
FLOOR = -1e30
HIGHEST = lax.Precision.HIGHEST
STATE_ROWS = BLOCK + 16


def dot(a, b, dims=((1,), (0,)), precision=None):
    return lax.dot_general(a, b, (dims, ((), ())), precision=precision, preferred_element_type=F32)


def split(x):
    high = x.astype(BF16)
    return high, (x - high.astype(F32)).astype(BF16)


def visits(nz):
    order = []
    for d in range(2, nz // 2 + 1):
        order += [d] if 2 * d == nz else [d, -d]
    return order + ([1] if nz == 2 else [-1, 1]) + [0]


def merge(earlier, later):
    peak = jnp.maximum(later[2] + earlier[1], later[1])
    fade_earlier = jnp.exp(later[2] + earlier[1] - peak)
    fade_later = jnp.exp(later[1] - peak)
    return (fade_earlier * earlier[0] + fade_later * later[0], peak, earlier[2] + later[2])


def identity(depth=BLOCK):
    return (
        jnp.zeros((depth, BLOCK), F32),
        jnp.full((1, BLOCK), FLOOR, F32),
        jnp.zeros((1, BLOCK), F32),
    )


def load_state(ref, n):
    depth = ref.shape[1] - 16
    return ref[n, 0:depth, :], ref[n, depth : depth + 1, :], ref[n, depth + 8 : depth + 9, :]


def store_state(ref, n, state):
    depth = ref.shape[1] - 16
    ref[n, 0:depth, :] = state[0]
    ref[n, depth : depth + 8, :] = jnp.broadcast_to(state[1], (8, BLOCK))
    ref[n, depth + 8 : depth + 16, :] = jnp.broadcast_to(state[2], (8, BLOCK))


def chosen(pred, a, b):
    return tuple(jnp.where(pred, s, t) for s, t in zip(a, b))


def log_sigmoid(x):
    small = jnp.exp(-jnp.abs(x))
    whole = 1.0 + small
    direct = jnp.log(whole) + (small - (whole - 1.0)) / whole
    series = small * (
        1.0 - small * (0.5 - small * (1.0 / 3.0 - small * (0.25 - small * (0.2 - small / 6.0))))
    )
    return jnp.minimum(x, 0.0) - jnp.where(small < 1.0 / 64.0, series, direct)


def norm_rows(src, dst, gain, rows, step, base=0):
    def body(i, carry):
        at = pl.ds(pl.multiple_of(base + i * step, step), step)
        wide = src[at, :].astype(F32)
        scaled = wide * lax.rsqrt(jnp.mean(wide * wide, axis=-1, keepdims=True) + EPSILON)
        dst[at, :] = (scaled * gain[...]).astype(BF16)
        return carry

    lax.fori_loop(0, rows // step, body, 0)


def kernel(dims, *refs):
    nz, ny, nx = dims.nz, dims.ny, dims.nx
    r = SimpleNamespace(**dict(zip(dims.names, refs)))
    plane = ny * CORES
    n_ep = nz * plane
    tokens = r.x_b.shape[0]
    width = r.x_b.shape[1]
    share = width // nx
    slots = r.outg.shape[0]
    cap = slots // n_ep
    chunk = plane * cap
    half = chunk // 2
    hid_w = r.gate.shape[1]
    heads = r.i_gate.shape[0]
    rows_a = r.x_a.shape[0]
    blocks = rows_a // BLOCK
    scale = BLOCK ** (-0.5)

    ep = lax.axis_index("ep")
    x = lax.axis_index("tp")
    z = lax.div(ep, plane)
    y = lax.div(lax.rem(ep, plane), CORES)
    c = lax.rem(ep, CORES)
    order = visits(nz)
    wide_from = nz - dims.near

    def offset(j):
        total = 0
        for k, d in enumerate(order):
            total = jnp.where(j == k, d, total)
        return total

    right = lax.rem(x + 1, nx)
    left = lax.rem(x + nx - 1, nx)
    mate = ep + 1 - 2 * c

    def rows(at, count, unit):
        return pl.ds(pl.multiple_of(at, unit), count)

    def remote(src, dst, send, recv, to_ep, to_x):
        return pltpu.make_async_remote_copy(
            src_ref=src,
            dst_ref=dst,
            send_sem=send,
            recv_sem=recv,
            device_id=(to_ep, to_x),
            device_id_type=MESH,
        )

    def settle(view, sem):
        pltpu.make_async_copy(view, view, sem).wait()

    barrier = pltpu.get_barrier_semaphore()

    def greet(k, carry):
        to = lax.rem(ep + k, n_ep)
        pl.semaphore_signal(barrier, inc=1, device_id=(to, x), device_id_type=MESH)
        return carry

    lax.fori_loop(1, n_ep, greet, 0)
    for k in range(1, nx):
        to = lax.rem(x + k, nx)
        pl.semaphore_signal(barrier, inc=1, device_id=(ep, to), device_id_type=MESH)

    down_at = r.down_h.at[:, rows(x * share, share, 128)]
    loads = SimpleNamespace()
    for n, (name, pair) in enumerate(
        dict(
            x_b=(r.x_b, r.xb),
            x_a=(r.x_a, r.xa),
            wq=(r.wq_h, r.wq),
            wk=(r.wk_h, r.wk),
            wv=(r.wv_h, r.wv),
            gate=(r.gate_h, r.gate),
            up=(r.up_h, r.up),
            group=(r.group_h, r.group),
            expert=(r.expert_h, r.expert),
            down=(down_at, r.down.at[x]),
            wout=(r.wout_h, r.wout.at[x]),
        ).items()
    ):
        load = pltpu.make_async_copy(*pair, r.load_s.at[n])
        setattr(loads, name, load)
    loads.x_b.start()

    route_rows = r.routes[...]
    experts_iota = lax.broadcasted_iota(jnp.int32, (n_ep, tokens), 0)
    hit0 = experts_iota == route_rows[0:1, :]
    hit1 = experts_iota == route_rows[1:2, :]
    named = jnp.where(hit0, 1.0, 0.0) + jnp.where(hit1, 1.0, 0.0)
    before = jnp.where(
        lax.broadcasted_iota(jnp.int32, (tokens, tokens), 0)
        < lax.broadcasted_iota(jnp.int32, (tokens, tokens), 1),
        1.0,
        0.0,
    ).astype(BF16)
    counts = dot(named.astype(BF16), before)
    place0 = jnp.sum(jnp.where(hit0, counts, 0.0), axis=0, keepdims=True)
    place1 = jnp.sum(jnp.where(hit1, counts, 0.0), axis=0, keepdims=True)
    route0 = route_rows[0:1, :].astype(F32)
    route1 = route_rows[1:2, :].astype(F32)
    slot0 = route0 * cap + place0
    slot1 = route1 * cap + place1
    flip = r.flip
    flip[...] = jnp.zeros_like(flip)
    flip[0:1, :] = route0
    flip[1:2, :] = route1
    flip[2:3, :] = slot0
    flip[3:4, :] = slot1
    r.cols[...] = jnp.transpose(flip[...])

    loads.x_b.wait()
    for load in list(vars(loads).values())[1:]:
        load.start()
    norm_rows(r.xb, r.nb, r.gain_b, tokens, min(32, tokens))

    def packed(j, wide):
        z_to = lax.rem(z - offset(j) + nz, nz)
        base = z_to * chunk
        place = (lax.broadcasted_iota(jnp.int32, (chunk, tokens), 0) + base).astype(F32)
        taken = jnp.where(place == flip[2:3, :], 1.0, 0.0) + jnp.where(
            place == flip[3:4, :], 1.0, 0.0
        )
        taken = taken.astype(BF16)
        if wide:
            for q in range(nx):
                part = r.nb[:, q * share : (q + 1) * share]
                r.near[j - wide_from, q, :, :] = dot(taken, part).astype(BF16)
        else:
            own = r.nb[:, rows(x * share, share, 128)]
            r.outg[rows(base, chunk, chunk), :] = dot(taken, own).astype(BF16)

    def pack_near(j, carry):
        packed(j, True)
        return carry

    def pack_far(j, carry):
        packed(j, False)
        return carry

    lax.fori_loop(0, wide_from, pack_far, 0)
    lax.fori_loop(wide_from, nz, pack_near, 0)

    pl.semaphore_wait(barrier, n_ep - 1 + nx - 1)

    far = lax.rem(x + 2, nx)
    fold = hid_w // 2
    for k, to in enumerate((right, left)):
        remote(
            r.down_h.at[:, rows(to * share, share, 128)],
            r.down.at[x],
            r.down_ss.at[k],
            r.down_rs.at[x],
            ep,
            to,
        ).start()
    for k, to in enumerate((right, left)):
        remote(
            r.down_h.at[k * fold : (k + 1) * fold, rows(far * share, share, 128)],
            r.relay.at[k],
            r.down_ss.at[2 + k],
            r.relay_rs.at[k],
            ep,
            to,
        ).start()

    def pass_down():
        for k, (source_x, to) in enumerate(((left, right), (right, left))):
            settle(r.relay.at[k], r.relay_rs.at[k])
            remote(
                r.relay.at[k],
                r.down.at[source_x, k * fold : (k + 1) * fold, :],
                r.down_ss.at[4 + k],
                r.far_rs.at[k],
                ep,
                to,
            ).start()

    def posted(j, wide):
        z_to = lax.rem(z - offset(j) + nz, nz)

        def post(k, inner):
            to = z_to * plane + k

            @pl.when(to != ep)
            def _():
                if wide:
                    src = r.near.at[j - wide_from, :, rows(k * cap, cap, cap), :]
                    dst = r.tok.at[:, rows(ep * cap, cap, cap), :]
                else:
                    src = r.outg.at[rows(to * cap, cap, cap), :]
                    dst = r.tok.at[x, rows(ep * cap, cap, cap), :]
                remote(src, dst, r.disp_ss.at[z_to], r.disp_rs.at[z], to, x).start()

            return inner

        lax.fori_loop(0, plane, post, 0)

    def post_near(j, carry):
        posted(j, True)
        return carry

    def post_far(j, carry):
        posted(j, False)
        return carry

    lax.fori_loop(0, wide_from, post_far, 0)
    lax.fori_loop(wide_from, nz, post_near, 0)
    own_rows = rows(ep * cap, cap, cap)
    own_place = rows(lax.rem(ep, plane) * cap, cap, cap)
    kept = pltpu.make_async_copy(
        r.near.at[dims.near - 1, :, own_place, :], r.tok.at[:, own_rows, :], r.kept_s.at[0]
    )
    kept.start()

    def ring_of(me, count, device):
        after, ahead = lax.rem(me + 1, count), lax.rem(me + count - 1, count)
        return SimpleNamespace(
            me=me,
            right=after,
            left=ahead,
            far=lax.rem(me + 2, count),
            to_right=device(after),
            to_left=device(ahead),
        )

    over_x = ring_of(x, nx, lambda to: (ep, to))
    over_y = ring_of(y, ny, lambda to: (z * plane + to * CORES + c, x))

    def ring_start(ring, view, src, ss, rs, j):
        remote(src, view(ring.me), ss.at[0, j], rs.at[0, j], *ring.to_right).start()
        remote(src, view(ring.me), ss.at[1, j], rs.at[1, j], *ring.to_left).start()

    def ring_forward(ring, view, low, high, ss, rs, j):
        settle(view(ring.left), rs.at[0, j])
        part = low(ring.left)
        remote(part, part, ss.at[2, j], rs.at[2, j], *ring.to_right).start()
        settle(view(ring.right), rs.at[1, j])
        part = high(ring.right)
        remote(part, part, ss.at[3, j], rs.at[3, j], *ring.to_left).start()

    def ring_finish(ring, low, high, rs, j):
        settle(low(ring.far), rs.at[2, j])
        settle(high(ring.far), rs.at[3, j])

    def ring_sent(ring, view, low, high, ss, j):
        settle(view(ring.me), ss.at[0, j])
        settle(view(ring.me), ss.at[1, j])
        settle(low(ring.left), ss.at[2, j])
        settle(high(ring.right), ss.at[3, j])

    def source(j):
        return lax.rem(z + offset(j) + nz, nz)

    def tok_views(j):
        base = source(j) * chunk
        return (
            lambda q: r.tok.at[q, rows(base, chunk, chunk), :],
            lambda q: r.tok.at[q, rows(base, half, half), :],
            lambda q: r.tok.at[q, rows(base + half, half, half), :],
        )

    def hid_views(j):
        base = source(j) * chunk
        return (
            lambda q: r.hid.at[q, rows(base, chunk, chunk), :],
            lambda q: r.hid.at[q, rows(base, half, half), :],
            lambda q: r.hid.at[q, rows(base + half, half, half), :],
        )

    out_half = r.wout.shape[1] // CORES
    out_part = out_half // ny

    def wout_views(q=None):
        def cut(base, count):
            def view(n):
                at, place = (n, y) if q is None else (q, n)
                return r.wout.at[at, rows(c * out_half + place * out_part + base, count, 16), :]

            return view

        return cut(0, out_part), cut(0, out_part // 2), cut(out_part // 2, out_part // 2)

    others = [lax.rem(x + k, nx) for k in range(1, nx)]

    def wout_half(q):
        return r.wout.at[q, rows(c * out_half, out_half, out_half), :]

    def take_rows(j):
        view, low, high = tok_views(j)
        settle(view(x), r.disp_rs.at[source(j)])
        ring_start(over_x, view, view(x), r.tok_ss, r.tok_rs, j)

    def expand(j):
        view, low, high = tok_views(j)
        at = rows(source(j) * chunk, chunk, chunk)

        @pl.when(j == nz - 1)
        def _():
            settle(r.near.at[0, :, rows(0, chunk - cap, cap), :], r.disp_rs.at[z])
            kept.wait()

        @pl.when(jnp.logical_and(j >= wide_from, j < nz - 1))
        def _():
            settle(r.tok.at[:, at, :], r.disp_rs.at[source(j)])

        @pl.when(j < wide_from)
        def _():
            ring_finish(over_x, low, high, r.tok_rs, j)

        gated = jnp.zeros((chunk, hid_w), F32)
        upped = jnp.zeros((chunk, hid_w), F32)
        for q in range(nx):
            part = r.tok[q, at, :]
            gated += dot(part, r.gate[q * share : (q + 1) * share, :])
            upped += dot(part, r.up[q * share : (q + 1) * share, :])
        r.hid[x, at, :] = (gated * jax.nn.sigmoid(gated) * upped).astype(BF16)
        hview = hid_views(j)[0]
        ring_start(over_x, hview, hview(x), r.hid_ss, r.hid_rs, j)

    def contract(j):
        view, low, high = hid_views(j)
        ring_finish(over_x, low, high, r.hid_rs, j)
        z_to = source(j)
        at = rows(z_to * chunk, chunk, chunk)
        total = jnp.zeros((chunk, share), F32)
        for q in range(nx):
            total += dot(r.hid[q, at, :], r.down[q]).astype(BF16).astype(F32)
        r.res[at, :] = total.astype(BF16)

        def post(k, inner):
            to = z_to * plane + k

            @pl.when(to != ep)
            def _():
                remote(
                    r.res.at[rows(to * cap, cap, cap), :],
                    r.ret.at[rows(ep * cap, cap, cap), :],
                    r.ret_ss.at[z_to],
                    r.ret_rs.at[z],
                    to,
                    x,
                ).start()

            return inner

        lax.fori_loop(0, plane, post, 0)

        @pl.when(j == nz - 1)
        def _():
            pltpu.make_async_copy(
                r.res.at[own_rows, :], r.ret.at[own_rows, :], r.kept_s.at[1]
            ).start()

    def gather_up(j):
        z_from = lax.rem(z - offset(j) + nz, nz)
        base = z_from * chunk
        at = rows(base, chunk, chunk)

        @pl.when(j == 0)
        def _():
            r.acc[...] = jnp.zeros_like(r.acc)

        @pl.when(j == nz - 1)
        def _():
            settle(r.res.at[rows(0, chunk - cap, cap), :], r.ret_rs.at[z])
            settle(r.res.at[rows(0, cap, cap), :], r.kept_s.at[1])

        @pl.when(j < nz - 1)
        def _():
            settle(r.ret.at[at, :], r.ret_rs.at[z_from])

        lane = (lax.broadcasted_iota(jnp.int32, (tokens, chunk), 1) + base).astype(F32)
        back = r.ret[at, :]
        for k in range(2):
            picks = jnp.where(lane == r.cols[:, 2 + k : 3 + k], 1.0, 0.0).astype(BF16)
            r.acc[...] += r.comb[:, k : k + 1] * dot(picks, back)

    def weights():
        loads.group.wait()
        loads.expert.wait()
        normed = r.nb[...]
        group_logits = dot(normed, r.group[...], ((1,), (1,)))
        expert_logits = dot(normed, r.expert[...], ((1,), (1,)))
        members = expert_logits.shape[1] // group_logits.shape[1]
        groups_iota = lax.broadcasted_iota(jnp.int32, group_logits.shape, 1)
        lanes_iota = lax.broadcasted_iota(jnp.int32, expert_logits.shape, 1)
        picked, grouped = [], []
        for k in range(2):
            route = r.cols[:, k : k + 1].astype(jnp.int32)
            picked.append(
                jnp.sum(jnp.where(lanes_iota == route, expert_logits, 0.0), axis=1, keepdims=True)
            )
            first = route - groups_iota * members
            inside = jnp.logical_and(first >= 0, first < members)
            grouped.append(jnp.sum(jnp.where(inside, group_logits, 0.0), axis=1, keepdims=True))
        for k in range(2):
            r.comb[:, k : k + 1] = jax.nn.sigmoid(grouped[k]) * jax.nn.sigmoid(
                picked[k] - picked[1 - k]
            )

    def project(first, last):
        if first == 0:
            loads.x_a.wait()
            loads.wq.wait()
            loads.wk.wait()
            loads.wv.wait()

        def body(b, carry):
            at = rows(b * BLOCK, BLOCK, BLOCK)
            norm_rows(r.xa, r.na, r.gain_a, BLOCK, 32, b * BLOCK)
            normed = r.na[at, :]
            for weight, to in ((r.wq, r.q), (r.wk, r.k), (r.wv, r.v)):
                to[at, :] = dot(normed, weight[...]).astype(BF16)
            return carry

        lax.fori_loop(first, last, body, 0)

    def pieces(n):
        h, b = n // blocks, n % blocks
        at = (slice(b * BLOCK, (b + 1) * BLOCK), slice(h * BLOCK, (h + 1) * BLOCK))
        return r.q[at], r.k[at], r.v[at]

    def summarize():
        logs = log_sigmoid(r.f_gate[...])
        inputs = r.i_gate[...]
        gates = r.gates
        for n in range(heads * blocks):
            h, b = n // blocks, n % blocks
            lanes = slice(b * BLOCK, (b + 1) * BLOCK)
            gates[n : n + 1, :] = logs[h : h + 1, lanes]
            gates[16 + n : 17 + n, :] = inputs[h : h + 1, lanes]
        upto = jnp.where(
            lax.broadcasted_iota(jnp.int32, (BLOCK, BLOCK), 0)
            <= lax.broadcasted_iota(jnp.int32, (BLOCK, BLOCK), 1),
            1.0,
            0.0,
        )
        count = heads * blocks
        sums = dot(gates[0:count, :], upto, precision=HIGHEST)
        totals = sums[:, BLOCK - 1 : BLOCK]
        log_weight = totals - sums + gates[16 : 16 + count, :]
        peaks = jnp.max(log_weight, axis=1, keepdims=True)
        turn = r.turn
        turn[...] = jnp.zeros_like(turn)
        turn[0:count, :] = sums
        turn[count : 2 * count, :] = jnp.exp(log_weight - peaks)
        turned = jnp.transpose(turn[...])
        r.turned[...] = turned
        for h in range(heads):
            summary = None
            for b in range(blocks):
                n = h * blocks + b
                _, keys, values = pieces(n)
                high, low = split(values.astype(F32) * turned[:, count + n : count + n + 1])
                memory = scale * (dot(keys, high, ((0,), (0,))) + dot(keys, low, ((0,), (0,))))
                state = (
                    memory,
                    jnp.broadcast_to(peaks[n : n + 1, :], (1, BLOCK)),
                    jnp.broadcast_to(totals[n : n + 1, :], (1, BLOCK)),
                )
                store_state(r.sums, n, state)
                summary = state if summary is None else merge(summary, state)
            store_state(r.own, h, summary)
        remote(r.own, r.other, r.mate_ss.at[0], r.mate_rs.at[0], mate, x).start()

    def chip_level():
        settle(r.other, r.mate_rs.at[0])
        mine, theirs = load_state(r.own, c), load_state(r.other, c)
        first = c == 0
        store_state(
            r.y_in, y, merge(chosen(first, mine, theirs), chosen(first, theirs, mine))
        )
        for k in range(1, ny):
            y_to = lax.rem(y + k, ny)
            remote(
                r.y_in.at[y],
                r.y_in.at[y],
                r.y_ss.at[k],
                r.y_rs.at[y],
                z * plane + y_to * CORES + c,
                x,
            ).start()

    def run_up(ref, count, place, run):
        depth = run.shape[1] - 16
        store_state(run, 0, identity(depth))
        store_state(run, 1, identity(depth))

        def body(k, carry):
            after = merge(load_state(run, 1), load_state(ref, k))

            store_state(run, 1, after)

            @pl.when(k + 1 == place)
            def _():
                store_state(run, 0, after)

            return carry

        lax.fori_loop(0, count, body, 0)

    def plane_level():
        for k in range(1, ny):
            y_from = lax.rem(y + k, ny)
            settle(r.y_in.at[y_from], r.y_rs.at[y_from])
        run_up(r.y_in, ny, y, r.y_run)
        _, peak, total = load_state(r.y_run, 1)
        part = r.z_in.shape[1] - 16
        store_state(r.z_in, z, (r.y_run[1, rows(y * part, part, part), :], peak, total))
        for k in range(1, nz):
            z_to = lax.rem(z + k, nz)
            remote(
                r.z_in.at[z],
                r.z_in.at[z],
                r.z_ss.at[k],
                r.z_rs.at[z],
                z_to * plane + y * CORES + c,
                x,
            ).start()

    def line_level():
        for k in range(1, nz):
            z_from = lax.rem(z + k, nz)
            settle(r.z_in.at[z_from], r.z_rs.at[z_from])
        run_up(r.z_in, nz, z, r.z_run)
        store_state(r.line, y, load_state(r.z_run, 0))
        for k in range(1, ny):
            y_to = lax.rem(y + k, ny)
            remote(
                r.line.at[y],
                r.line.at[y],
                r.line_ss.at[k],
                r.line_rs.at[y],
                z * plane + y_to * CORES + c,
                x,
            ).start()

    def start_level():
        for k in range(1, ny):
            y_from = lax.rem(y + k, ny)
            settle(r.line.at[y_from], r.line_rs.at[y_from])
        parts = [load_state(r.line, k) for k in range(ny)]
        memory = jnp.concatenate([part[0] for part in parts], axis=0)
        store_state(r.start, c, merge((memory, *parts[0][1:]), load_state(r.y_run, 0)))
        remote(
            r.start.at[c],
            r.start.at[c],
            r.mate_ss.at[1],
            r.mate_rs.at[1],
            mate,
            x,
        ).start()

    def attend(first, last):
        if first == 0:
            settle(r.start.at[1 - c], r.mate_rs.at[1])
        count = heads * blocks
        turned = r.turned
        gates = r.gates
        states = []
        for h in range(heads):
            if first == 0:
                later = chosen(c == 1, load_state(r.other, h), identity())
                states.append(merge(load_state(r.start, h), later))
            else:
                states.append(load_state(r.current, h))
        causal = lax.broadcasted_iota(jnp.int32, (BLOCK, BLOCK), 0) >= lax.broadcasted_iota(
            jnp.int32, (BLOCK, BLOCK), 1
        )
        for b in range(first, last):
            for h in range(heads):
                n = h * blocks + b
                queries, keys, values = pieces(n)
                memory, peak, _ = states[h]
                column = turned[:, n : n + 1]
                within = column - r.turn[n : n + 1, :] + gates[16 + n : 17 + n, :]
                within = jnp.where(causal, within, FLOOR)
                carried = column + peak[:, 0:1]
                top = jnp.maximum(jnp.max(within, axis=1, keepdims=True), carried)
                raw = dot(queries, keys, ((1,), (1,))) * scale
                scores = (raw * jnp.exp(within - top)).astype(BF16)
                high, low = split(memory)
                recalled = dot(queries, high) + dot(queries, low)
                cells = dot(scores, values) + jnp.exp(carried - top) * recalled
                square = jnp.mean(cells * cells, axis=1, keepdims=True)
                gain = r.gain_h[pl.ds(x * heads + h, 1), :]
                r.cell[b, :, h * BLOCK : (h + 1) * BLOCK] = (
                    cells * lax.rsqrt(square + EPSILON) * gain
                ).astype(BF16)
                if b + 1 < blocks:
                    states[h] = merge(states[h], load_state(r.sums, n))
        if last < blocks:
            for h in range(heads):
                store_state(r.current, h, states[h])
            return
        for k in range(1, nx):
            to = lax.rem(x + k, nx)
            remote(
                r.cell.at[to],
                r.cells.at[x],
                r.cell_ss.at[k],
                r.cell_rs.at[x],
                ep,
                to,
            ).start()
        r.cells[x] = r.cell[x]

    def mix_out():
        for k in range(1, nx):
            q = lax.rem(x + k, nx)
            settle(r.cells.at[q], r.cell_rs.at[q])
            other_half = rows((1 - c) * out_half, out_half, out_half)
            settle(r.wout.at[q, other_half, :], r.wm_rs.at[q])
        loads.wout.wait()
        step = r.mixed.shape[1] // 4
        for n in range(4):
            lanes = slice(n * step, (n + 1) * step)
            total = jnp.zeros((BLOCK, step), F32)
            for g in range(nx):
                total += dot(r.cells[g], r.wout[g, :, lanes]).astype(BF16).astype(F32)
            r.mixed[:, lanes] = total.astype(BF16)
        pltpu.make_async_copy(r.mixed, r.out_a, r.out_s.at[0]).start()

    when, lag = dims.when, dims.lag

    def at_step(number, job):
        @pl.when(jnp.logical_and(number >= 0, number < nz))
        def _():
            job(number)

    def far_only(job):
        def run(j):
            @pl.when(j < wide_from)
            def _():
                job(j)

        return run

    def forward_rows(j):
        ring_forward(over_x, *tok_views(j), r.tok_ss, r.tok_rs, j)

    def forward_hidden(j):
        ring_forward(over_x, *hid_views(j), r.hid_ss, r.hid_rs, j)

    def down_arrived():
        loads.down.wait()
        for k, source_x in enumerate((left, right)):
            settle(r.down.at[source_x], r.down_rs.at[source_x])
            settle(r.relay.at[k], r.far_rs.at[k])

    def experts_arrived():
        loads.gate.wait()
        loads.up.wait()

    def wout_start():
        own = r.wout_h.at[rows(c * out_half + y * out_part, out_part, 16), :]
        ring_start(over_x, wout_views()[0], own, r.w_ss, r.w_rs, 0)

    def wout_forward():
        ring_forward(over_x, *wout_views(), r.w_ss, r.w_rs, 0)

    def wout_turn():
        ring_finish(over_x, *wout_views()[1:], r.w_rs, 0)
        for k, q in enumerate(others):
            view = wout_views(q)[0]
            ring_start(over_y, view, view(y), r.wy_ss, r.wy_rs, k)

    def wout_pass():
        for k, q in enumerate(others):
            ring_forward(over_y, *wout_views(q), r.wy_ss, r.wy_rs, k)

    def wout_spread():
        for k, q in enumerate(others):
            ring_finish(over_y, *wout_views(q)[1:], r.wy_rs, k)
            half = wout_half(q)
            remote(half, half, r.wm_ss.at[k], r.wm_rs.at[q], mate, x).start()

    first_jobs = ((lag.expand, experts_arrived), (lag.contract, down_arrived))
    jobs = (
        (when.pass_down, pass_down),
        (when.wout_start, wout_start),
        (when.chip, chip_level),
        (when.plane, plane_level),
        (when.wout_forward, wout_forward),
        (when.line, line_level),
        (when.start, start_level),
        (when.weights, weights),
        (when.attend, functools.partial(attend, 0, blocks // 2)),
        (when.attend + 1, functools.partial(attend, blocks // 2, blocks)),
        (when.wout_turn, wout_turn),
        (when.wout_pass, wout_pass),
        (when.wout_spread, wout_spread),
        (when.mix, mix_out),
    )
    project(0, blocks)
    summarize()

    def step(i, carry):
        at_step(i - lag.take, far_only(take_rows))
        at_step(i - lag.forward, far_only(forward_rows))
        for place, job in first_jobs:
            pl.when(i == place)(job)
        at_step(i - lag.expand, expand)
        at_step(i - lag.hidden, forward_hidden)
        at_step(i - lag.contract, contract)
        at_step(i - lag.gather, gather_up)
        for place, job in jobs:
            pl.when(i == place)(job)
        return carry

    lax.fori_loop(min(0, lag.take), max(nz + lag.gather, when.mix + 1), step, 0)

    r.mixed_b[...] = r.acc[...].astype(BF16)
    last = pltpu.make_async_copy(r.mixed_b, r.out_b, r.out_s.at[1])
    last.start()

    def sent(j, carry):
        z_to = lax.rem(z - offset(j) + nz, nz)
        ring_sent(over_x, *hid_views(j), r.hid_ss, j)

        @pl.when(j == nz - 1)
        def _():
            settle(r.near.at[0, :, rows(0, chunk - cap, cap), :], r.disp_ss.at[z])
            settle(r.res.at[rows(0, chunk - cap, cap), :], r.ret_ss.at[z])

        @pl.when(j < nz - 1)
        def _():
            settle(r.res.at[rows(0, chunk, chunk), :], r.ret_ss.at[z_to])

        @pl.when(jnp.logical_and(j >= wide_from, j < nz - 1))
        def _():
            settle(r.near.at[0], r.disp_ss.at[z_to])

        @pl.when(j < wide_from)
        def _():
            settle(r.outg.at[rows(0, chunk, chunk), :], r.disp_ss.at[z_to])
            ring_sent(over_x, *tok_views(j), r.tok_ss, j)

        return carry

    lax.fori_loop(0, nz, sent, 0)
    ring_sent(over_x, *wout_views(), r.w_ss, 0)
    for k, q in enumerate(others):
        ring_sent(over_y, *wout_views(q), r.wy_ss, k)
        settle(wout_half(q), r.wm_ss.at[k])
        settle(r.cell.at[x], r.cell_ss.at[k + 1])
    for k in range(2):
        settle(r.down.at[x], r.down_ss.at[k])
        settle(r.relay.at[0], r.down_ss.at[k + 2])
        settle(r.relay.at[0], r.down_ss.at[k + 4])
    for k in range(1, ny):
        settle(r.y_in.at[y], r.y_ss.at[k])
        settle(r.line.at[y], r.line_ss.at[k])
    for k in range(1, nz):
        settle(r.z_in.at[z], r.z_ss.at[k])
    settle(r.own, r.mate_ss.at[0])
    settle(r.start.at[c], r.mate_ss.at[1])
    settle(r.mixed, r.out_s.at[0])
    last.wait()


def hand_out(a, b, out_a, out_b, held_a, held_b, sems):
    reads = [
        pltpu.make_async_copy(a, held_a, sems.at[0]),
        pltpu.make_async_copy(b, held_b, sems.at[1]),
    ]
    writes = [
        pltpu.make_async_copy(held_a, out_a, sems.at[2]),
        pltpu.make_async_copy(held_b, out_b, sems.at[3]),
    ]
    for read in reads:
        read.start()
    for read, write in zip(reads, writes):
        read.wait()
        write.start()
    for write in writes:
        write.wait()


def solution(mesh, shape=(8, 4)):
    nz, ny = shape
    nx = mesh.shape["tp"]
    n_ep = mesh.shape["ep"]

    def shards(
        mixer_in,
        mixer_gain,
        query_weight,
        key_weight,
        value_weight,
        input_gate,
        forget_gate,
        head_gain,
        mixer_out_weight,
        expert_in,
        expert_gain,
        group_router,
        expert_router,
        routes,
        gate_experts,
        up_experts,
        down_experts,
    ):
        rows_a, width = mixer_in.shape
        near = min(NEAR, nz - 1)
        tokens = expert_in.shape[0]
        share = width // nx
        cap = 4 * tokens // n_ep
        slots = n_ep * cap
        heads = input_gate.shape[0]
        blocks = rows_a // BLOCK
        qkv = query_weight.shape[1]
        hid_w = gate_experts.shape[2]
        vmem = pl.BlockSpec(memory_space=pltpu.VMEM)
        hbm = pl.BlockSpec(memory_space=pl.ANY)
        inputs = dict(
            x_a=(mixer_in, hbm),
            gain_a=(mixer_gain.reshape(1, -1), vmem),
            wq_h=(query_weight, hbm),
            wk_h=(key_weight, hbm),
            wv_h=(value_weight, hbm),
            i_gate=(input_gate, vmem),
            f_gate=(forget_gate, vmem),
            gain_h=(head_gain.reshape(-1, BLOCK), vmem),
            wout_h=(mixer_out_weight, hbm),
            x_b=(expert_in, hbm),
            gain_b=(expert_gain.reshape(1, -1), vmem),
            group_h=(group_router.T, hbm),
            expert_h=(expert_router.T, hbm),
            routes=(routes.T, vmem),
            gate_h=(gate_experts[0], hbm),
            up_h=(up_experts[0], hbm),
            down_h=(down_experts[0], hbm),
        )
        state = (STATE_ROWS, BLOCK)
        part = (BLOCK // ny + 16, BLOCK)
        dma = pltpu.SemaphoreType.DMA
        scratch = dict(
            xa=pltpu.VMEM((rows_a, width), BF16),
            xb=pltpu.VMEM((tokens, width), BF16),
            wq=pltpu.VMEM(query_weight.shape, BF16),
            wk=pltpu.VMEM(query_weight.shape, BF16),
            wv=pltpu.VMEM(query_weight.shape, BF16),
            gate=pltpu.VMEM((width, hid_w), BF16),
            up=pltpu.VMEM((width, hid_w), BF16),
            group=pltpu.VMEM(group_router.shape[::-1], BF16),
            expert=pltpu.VMEM(expert_router.shape[::-1], BF16),
            down=pltpu.VMEM((nx, hid_w, share), BF16),
            relay=pltpu.VMEM((2, hid_w // 2, share), BF16),
            wout=pltpu.VMEM((nx, qkv, mixer_out_weight.shape[1]), BF16),
            flip=pltpu.VMEM((128, tokens), F32),
            cols=pltpu.VMEM((tokens, 128), F32),
            nb=pltpu.VMEM((tokens, width), BF16),
            outg=pltpu.VMEM((slots, share), BF16),
            near=pltpu.VMEM((near, nx, slots // nz, share), BF16),
            tok=pltpu.VMEM((nx, slots, share), BF16),
            hid=pltpu.VMEM((nx, slots, hid_w), BF16),
            res=pltpu.VMEM((slots, share), BF16),
            ret=pltpu.VMEM((slots, share), BF16),
            comb=pltpu.VMEM((tokens, 128), F32),
            acc=pltpu.VMEM((tokens, share), F32),
            mixed_b=pltpu.VMEM((tokens, share), BF16),
            na=pltpu.VMEM((rows_a, width), BF16),
            q=pltpu.VMEM((rows_a, qkv), BF16),
            k=pltpu.VMEM((rows_a, qkv), BF16),
            v=pltpu.VMEM((rows_a, qkv), BF16),
            gates=pltpu.VMEM((32, BLOCK), F32),
            turn=pltpu.VMEM((BLOCK, BLOCK), F32),
            turned=pltpu.VMEM((BLOCK, BLOCK), F32),
            sums=pltpu.VMEM((heads * blocks, *state), F32),
            own=pltpu.VMEM((heads, *state), F32),
            other=pltpu.VMEM((heads, *state), F32),
            start=pltpu.VMEM((heads, *state), F32),
            current=pltpu.VMEM((heads, *state), F32),
            y_in=pltpu.VMEM((ny, *state), F32),
            y_run=pltpu.VMEM((2, *state), F32),
            z_in=pltpu.VMEM((nz, *part), F32),
            z_run=pltpu.VMEM((2, *part), F32),
            line=pltpu.VMEM((ny, *part), F32),
            cell=pltpu.VMEM((nx, BLOCK, qkv), BF16),
            cells=pltpu.VMEM((nx, BLOCK, qkv), BF16),
            mixed=pltpu.VMEM((BLOCK, width), BF16),
            load_s=dma((11,)),
            kept_s=dma((2,)),
            out_s=dma((2,)),
            down_ss=dma((6,)),
            relay_rs=dma((2,)),
            far_rs=dma((2,)),
            down_rs=dma((nx,)),
            disp_ss=dma((nz,)),
            disp_rs=dma((nz,)),
            tok_ss=dma((4, nz)),
            tok_rs=dma((4, nz)),
            hid_ss=dma((4, nz)),
            hid_rs=dma((4, nz)),
            ret_ss=dma((nz,)),
            ret_rs=dma((nz,)),
            w_ss=dma((4, 1)),
            w_rs=dma((4, 1)),
            wy_ss=dma((4, nx - 1)),
            wy_rs=dma((4, nx - 1)),
            wm_ss=dma((nx,)),
            wm_rs=dma((nx,)),
            mate_ss=dma((2,)),
            mate_rs=dma((2,)),
            y_ss=dma((ny,)),
            y_rs=dma((ny,)),
            line_ss=dma((ny,)),
            line_rs=dma((ny,)),
            z_ss=dma((nz,)),
            z_rs=dma((nz,)),
            cell_ss=dma((nx,)),
            cell_rs=dma((nx,)),
        )
        names = [*inputs, "out_a", "out_b", *scratch]
        when = SimpleNamespace(
            chip=0,
            plane=2,
            weights=3,
            line=6,
            start=8,
            attend=9,
            pass_down=1,
            wout_start=1,
            wout_forward=3,
            wout_turn=4,
            wout_pass=7,
            wout_spread=9,
            mix=12,
        )
        lag = SimpleNamespace(take=0, forward=1, expand=2, hidden=3, contract=4, gather=8)
        dims = SimpleNamespace(nz=nz, ny=ny, nx=nx, near=near, names=names, when=when, lag=lag)
        results = pl.pallas_call(
            functools.partial(kernel, dims),
            out_shape=(
                jax.ShapeDtypeStruct((rows_a // nx, width), BF16),
                jax.ShapeDtypeStruct((tokens, share), BF16),
            ),
            in_specs=[spec for _, spec in inputs.values()],
            out_specs=(hbm, hbm),
            scratch_shapes=list(scratch.values()),
            compiler_params=pltpu.CompilerParams(
                collective_id=0, has_side_effects=True, vmem_limit_bytes=60 * 1024 * 1024
            ),
            name="mixer_and_experts",
        )(*[value for value, _ in inputs.values()])
        return pl.pallas_call(
            hand_out,
            out_shape=[jax.ShapeDtypeStruct(part.shape, part.dtype) for part in results],
            in_specs=[hbm, hbm],
            out_specs=[hbm, hbm],
            scratch_shapes=[pltpu.VMEM(part.shape, part.dtype) for part in results] + [dma((4,))],
        )(*results)

    placed = (
        P("ep", None),
        P(),
        P(None, "tp"),
        P(None, "tp"),
        P(None, "tp"),
        P("tp", "ep"),
        P("tp", "ep"),
        P(),
        P("tp", None),
        P("ep", None),
        P(),
        P(),
        P(),
        P("ep", None),
        P("ep", None, "tp"),
        P("ep", None, "tp"),
        P("ep", "tp", None),
    )
    return jax.shard_map(
        shards,
        mesh=mesh,
        in_specs=placed,
        out_specs=(P(("ep", "tp"), None), P("ep", "tp")),
        check_vma=False,
    )
```
